32 devices in a mesh: fs: 8 (over z, y), tp: 4 (over x, core).
Axes of the slice: x: 2, y: 2, z: 4, core: 2. Of those that a mesh axis runs over, the one named last changes fastest.
Arguments:
- tokens: bfloat16 [8192, 2048], P('fs', 'tp'), may hold values from -6 to 6
- norm_gain: float32 [2048], P('fs'), may hold values from 0.1 to 1.9
- up_master: float32 [2048, 8192], P('fs', 'tp'), may hold values from -0.125 to 0.125
- down_master: float32 [2048, 8192], P('fs', 'tp'), may hold values from -0.0625 to 0.0625
Outputs:
- up_weights: bfloat16 [2048, 8192], P(None, 'tp')
- down_weights: bfloat16 [8192, 2048], P('tp')
- mlp_out: bfloat16 [8192, 2048], P('fs', 'tp')
The draws below stay inside these ranges and needn't reach their ends.
All inputs are finite; a program needn't handle non-finite values.
Results may differ from the reference program's by a relative error of at most 0.014.
Values may be sent and summed in bfloat16 or wider, within the bound.
A program may use at most 128 MiB of HBM per device.

```python
import jax
import jax.numpy as jnp
from jax import lax

D = 2048
FF = 8192
TOKENS = 8192
N_TP = 4


def block_scale(key, extent, cuts, smallest, high):
    loudness = 1.0
    for axis_at, parts in cuts:
        draws = jax.random.uniform(jax.random.fold_in(jax.random.fold_in(key, 6), axis_at), (parts,), jnp.float32, smallest / len(cuts), high / len(cuts))
        loudness = loudness * jnp.repeat(jnp.exp(draws), extent[axis_at] // parts).reshape((-1,) + (1,) * (len(extent) - 1 - axis_at))
    return loudness


def bell_draw(stream_key, shape, width, limit, shards=(), held_as=jnp.bfloat16):
    result = jax.random.normal(stream_key, shape, jnp.float32) * width
    if len(shards) > 0:
        result = block_scale(stream_key, shape, shards, -0.22, 0.18) * result
    return jnp.clip(result, min=-limit, max=limit).astype(held_as)


def setup_inputs(seed: int = 0) -> dict:
    key_list = jax.random.split(jax.random.key(seed), 5)
    tokens = bell_draw(key_list[0], (TOKENS, D), 1.0, 6.0, ((0, 8), (1, 4)))
    norm_gain = jnp.clip(1.0 + 0.18 * jax.random.normal(key_list[1], (D,), jnp.float32), 0.1, 1.9)
    up_master = bell_draw(key_list[2], (D, FF), D ** -0.5, 0.125, ((0, 8), (1, 4)), jnp.float32)
    down_master = bell_draw(key_list[3], (D, FF), FF ** -0.5, 0.0625, ((0, 8), (1, 4)), jnp.float32)
    return {"tokens": tokens, "norm_gain": norm_gain, "up_master": up_master, "down_master": down_master}


norm_floor = 1e-06

def reference(tokens, norm_gain, up_master, down_master):
    up_weights = (norm_gain[:, None] * up_master).astype(jnp.bfloat16)
    down_weights = jnp.transpose(down_master).astype(jnp.bfloat16)
    widened = tokens.astype(jnp.float32)
    normed = (widened * lax.rsqrt(lax.optimization_barrier(jnp.mean(widened * widened, axis=-1, keepdims=True)) + norm_floor)).astype(jnp.bfloat16)
    preact = jnp.dot(normed, up_weights, preferred_element_type=jnp.float32)
    hidden = jnp.square(jax.nn.relu(preact)).astype(jnp.bfloat16)
    block = FF // N_TP
    hidden_blocks = jnp.transpose(hidden.reshape(hidden.shape[0], N_TP, block), (1, 0, 2))
    down_blocks = down_weights.reshape(N_TP, block, D)

    def accumulate(total, pieces):
        partial_value = jnp.dot(pieces[0], pieces[1], preferred_element_type=jnp.float32).astype(jnp.bfloat16)
        partial_value = lax.optimization_barrier(partial_value)
        return (total + partial_value.astype(jnp.float32), None)
    start_total = jnp.zeros((hidden.shape[0], D), jnp.float32)
    total, unused = lax.scan(accumulate, start_total, (hidden_blocks, down_blocks))
    return (up_weights, down_weights, total.astype(jnp.bfloat16))
```

```python
import functools

import jax
import jax.numpy as jnp
from jax import lax
from jax.experimental import pallas as pl
from jax.experimental.pallas import tpu as pltpu
from jax.sharding import PartitionSpec as P

norm_floor = 1e-06
MESH = pl.DeviceIdType.MESH


def grid_of(n):
    ny = max(d for d in range(1, n + 1) if n % d == 0 and d * d <= n)
    return n // ny, ny


def position_of(f, nz, ny):
    if ny == 1:
        return f
    z, y = lax.div(f, ny), lax.rem(f, ny)
    tail = lax.div(y + (ny - 1), ny)
    k = nz - 1 - z
    odd = lax.rem(k, 2)
    r = (1 - odd) * (y - 1) + odd * (ny - 1 - y)
    return (1 - tail) * z + tail * (nz + k * (ny - 1) + r)


def index_at(p, nz, ny):
    if ny == 1:
        return p
    tail = lax.div(lax.div(p, nz) + (ny - 2), ny - 1)
    q = tail * (p - nz)
    k = lax.div(q, ny - 1)
    r = lax.rem(q, ny - 1)
    odd = lax.rem(k, 2)
    z = (1 - tail) * p + tail * (nz - 1 - k)
    y = tail * ((1 - odd) * (1 + r) + odd * (ny - 1 - r))
    return z * ny + y


def send_list(n):
    hops = n // 2
    split = n % 2 == 0

    def pieces(a, h):
        return [(a, h, 0)] if split and h == hops - 1 else [(a, h, 0), (a, h, 1)]

    ups = [p for h in range(1, hops) for p in pieces("u", h)]
    downs = [p for h in range(1, hops) for p in pieces("d", h)]
    own_u, own_d = pieces("u", 0), pieces("d", 0)
    return own_u + own_d[:1] + ups + own_d[1:] + downs


def gather_kernel(
    n_fs, n_tp, tokens, gain, up_l, dn_l, up_w, dn_w, recv, x, hid, part, stage, up_f, dn_f, gain_v,
    loc_sem, tok_s, tok_r, ring_s, ring_r, pre_s, pre_r, rs_s, rs_r,
):
    nz, ny = grid_of(n_fs)
    me_f, me_t = lax.axis_index("fs"), lax.axis_index("tp")
    pos = position_of(me_f, nz, ny)
    T, Dk = tokens.shape
    R, F = up_l.shape
    D = n_fs * R
    split_cols = (R // 2) % 128 == 0
    W = R // 2 if split_cols else R

    def at(offset):
        return index_at(lax.rem(pos + offset + n_fs, n_fs), nz, ny)

    right, left = at(1), at(-1)

    def tp_peer(k):
        return lax.rem(me_t + k, n_tp)

    barrier = pltpu.get_barrier_semaphore()
    for f in (right, left):
        pl.semaphore_signal(barrier, inc=1, device_id={"fs": f, "tp": me_t}, device_id_type=MESH)
    for k in range(1, n_tp):
        pl.semaphore_signal(barrier, inc=1, device_id={"fs": me_f, "tp": tp_peer(k)}, device_id_type=MESH)

    def up_piece(f, h):
        return up_w.at[pl.ds(pl.multiple_of(f * R + h * (R // 2), R // 2), R // 2), :]

    def dn_piece(f, h):
        if split_cols:
            return dn_w.at[:, pl.ds(pl.multiple_of(f * R + h * (R // 2), R // 2), R // 2)]
        return dn_w.at[pl.ds(h * (F // 2), F // 2), pl.ds(pl.multiple_of(f * R, R), R)]

    def tok_cols(t):
        return x.at[:, pl.ds(pl.multiple_of(t * Dk, Dk), Dk)]

    own = [
        pltpu.make_async_copy(up_l, up_f, loc_sem.at[0]),
        pltpu.make_async_copy(tokens, tok_cols(me_t), loc_sem.at[1]),
        pltpu.make_async_copy(dn_l, dn_f, loc_sem.at[2]),
    ]
    gain_copy = pltpu.make_async_copy(gain, gain_v, loc_sem.at[3])
    for c in [gain_copy] + own:
        c.start()
    own_rows = pl.ds(pl.multiple_of(me_f * R, R), R)
    gain_copy.wait()
    spread = jnp.transpose(jnp.broadcast_to(gain_v[...], (128, R)))
    own[0].wait()
    for c in range(F // 128):
        cols = pl.ds(c * 128, 128)
        up_w[own_rows, cols] = (spread * up_f[:, cols]).astype(jnp.bfloat16)
    own[1].wait()
    pl.semaphore_wait(barrier, n_tp + 1)

    order = send_list(n_fs)
    S = len(order)

    def ring_copy(s, d):
        a, hop, second = order[s]
        half = second if d == 0 else 1 - second
        f = at(-hop if d == 0 else hop)
        ref = up_piece(f, half) if a == "u" else dn_piece(f, half)
        return pltpu.make_async_remote_copy(
            src_ref=ref, dst_ref=ref, send_sem=ring_s.at[d, s], recv_sem=ring_r.at[d, s],
            device_id={"fs": right if d == 0 else left, "tp": me_t}, device_id_type=MESH,
        )

    def arrival(s, d):
        a, hop, second = order[s]
        half = second if d == 0 else 1 - second
        f = at(-(hop + 1) if d == 0 else hop + 1)
        return f, half, (up_piece(f, half) if a == "u" else dn_piece(f, half))

    def wait_arrival(s, d):
        f, half, ref = arrival(s, d)
        pltpu.make_async_remote_copy(
            src_ref=ref, dst_ref=ref, send_sem=ring_s.at[d, s], recv_sem=ring_r.at[d, s],
            device_id={"fs": right if d == 0 else left, "tp": me_t}, device_id_type=MESH,
        ).wait_recv()

    needs = [-1 if hop == 0 else order.index((a, hop - 1, second)) for a, hop, second in order]
    issued = [0]

    def issue(upto):
        while issued[0] < S and needs[issued[0]] <= upto:
            if upto < 0 and issued[0] >= 3:
                break
            for d in range(2):
                ring_copy(issued[0], d).start()
            issued[0] += 1

    for s in range(2):
        for d in range(2):
            ring_copy(s, d).start()

    def token_copy(k):
        return pltpu.make_async_remote_copy(
            src_ref=tok_cols(me_t), dst_ref=tok_cols(me_t), send_sem=tok_s.at[k], recv_sem=tok_r.at[k],
            device_id={"fs": me_f, "tp": tp_peer(k)}, device_id_type=MESH,
        )

    for k in range(1, n_tp):
        token_copy(k).start()
    own[2].wait()
    block = min(F, 256)

    @pl.loop(0, F // block)
    def _(i):
        r = pl.ds(pl.multiple_of(i * block, block), block)
        dn_w[r, own_rows] = jnp.transpose(dn_f[:, r]).astype(jnp.bfloat16)

    issued[0] = 2
    issue(-1)

    def normalise():
        for k in range(1, n_tp):
            src = lax.rem(me_t - k + n_tp, n_tp)
            pltpu.make_async_remote_copy(
                src_ref=tok_cols(src), dst_ref=tok_cols(src), send_sem=tok_s.at[k], recv_sem=tok_r.at[k],
                device_id={"fs": me_f, "tp": tp_peer(k)}, device_id_type=MESH,
            ).wait_recv()
            token_copy(k).wait_send()
        rows = 64

        @pl.loop(0, T // rows)
        def _(i):
            r = pl.ds(pl.multiple_of(i * rows, rows), rows)
            v = x[r, :].astype(jnp.float32)
            x[r, :] = (v * lax.rsqrt(jnp.mean(v * v, axis=-1, keepdims=True) + norm_floor)).astype(jnp.bfloat16)

    def make_hidden():
        width = 256

        @pl.loop(0, F // width)
        def _(i):
            c = pl.ds(pl.multiple_of(i * width, width), width)
            pre = jnp.dot(x[...], up_w[:, c], preferred_element_type=jnp.float32)
            hid[:, c] = jnp.square(jnp.maximum(pre, 0.0)).astype(jnp.bfloat16)

    per_owner = Dk // W
    nx = n_tp // 2
    half_rows = T // 2
    me_x, me_c = lax.div(me_t, 2), lax.rem(me_t, 2)
    sibling = me_t + 1 - 2 * me_c
    my_half = pl.ds(pl.multiple_of(me_c * half_rows, half_rows), half_rows)
    its_half = pl.ds(pl.multiple_of((1 - me_c) * half_rows, half_rows), half_rows)

    def device(t):
        return dict(device_id={"fs": me_f, "tp": t}, device_id_type=MESH)

    def cols_of(q):
        return pl.ds(pl.multiple_of(lax.rem(q, per_owner) * W, W), W)

    def whole_copy(q):
        return pltpu.make_async_remote_copy(
            src_ref=part.at[q], dst_ref=recv.at[nx, :, cols_of(q)],
            send_sem=rs_s.at[q], recv_sem=rs_r.at[nx, lax.rem(q, per_owner), 0], **device(sibling),
        )

    def pair_copy(q):
        return pltpu.make_async_remote_copy(
            src_ref=part.at[q, its_half], dst_ref=stage.at[q],
            send_sem=pre_s.at[q], recv_sem=pre_r.at[q], **device(sibling),
        )

    def half_copy(q):
        return pltpu.make_async_remote_copy(
            src_ref=part.at[q, my_half], dst_ref=recv.at[me_x, my_half, cols_of(q)],
            send_sem=rs_s.at[q], recv_sem=rs_r.at[me_x, lax.rem(q, per_owner), me_c],
            **device(lax.div(q, per_owner)),
        )

    def pass_on(q):
        @pl.when(lax.div(q, 2 * per_owner) != me_x)
        def _():
            pair_copy(q).wait_recv()
            both = part[q, my_half, :].astype(jnp.float32) + stage[q].astype(jnp.float32)
            part[q, my_half, :] = both.astype(jnp.bfloat16)
            half_copy(q).start()

    def do_parts(first, count):
        c = pl.ds(pl.multiple_of(first * W, W), count * W)

        @pl.loop(0, 2)
        def _(i):
            r = pl.ds(pl.multiple_of(lax.rem(i + 1 + me_c, 2) * half_rows, half_rows), half_rows)
            out = jnp.dot(hid[r, :], dn_w[:, c], preferred_element_type=jnp.float32).astype(jnp.bfloat16)
            for k in range(count):
                part[first + k, r, :] = out[:, k * W : (k + 1) * W]
            for k in range(count):
                owner = lax.div(first + k, per_owner)

                @pl.when((i == 0) & (lax.div(owner, 2) != me_x))
                def _():
                    pair_copy(first + k).start()

                @pl.when((i == 1) & (owner == sibling))
                def _():
                    whole_copy(first + k).start()

    per_chunk = R // W
    ready = [(me_f * per_chunk, per_chunk)]
    last_up = max(s for s in range(S) if order[s][0] == "u")
    norm_at = max(0, last_up - 2)
    for s in range(S):
        for d in range(2):
            wait_arrival(s, d)
        issue(s)
        a, hop, _ = order[s]
        if a == "d" and split_cols:
            if n_fs % 2 == 0 and hop == n_fs // 2 - 1:
                ready.append((at(hop + 1) * 2, 2))
            else:
                for d in range(2):
                    f, half, _ = arrival(s, d)
                    ready.append((f * 2 + half, 1))
        if s == norm_at:
            normalise()
        if s == last_up:
            make_hidden()
        if s >= last_up:
            for first, count in ready:
                do_parts(first, count)
            for first, count in ready:
                for k in range(count):
                    pass_on(first + k)
            ready = []
    if not split_cols:
        @pl.loop(0, n_fs)
        def _(q):
            @pl.when(q != me_f)
            def _():
                do_parts(q, 1)
                pass_on(q)

    @pl.loop(0, per_owner)
    def _(local):
        cols = pl.ds(pl.multiple_of(local * W, W), W)
        recv[me_x, :, cols] = part[me_t * per_owner + local]

    for d in range(2):
        for s in range(S):
            ring_copy(s, d).wait_send()

    @pl.loop(0, D // W)
    def _(q):
        owner = lax.div(q, per_owner)

        @pl.when(owner == sibling)
        def _():
            whole_copy(q).wait_send()

        @pl.when(lax.div(owner, 2) != me_x)
        def _():
            pair_copy(q).wait_send()
            half_copy(q).wait_send()

    for local in range(per_owner):
        q = me_t * per_owner + local
        whole_copy(q).wait_recv()
        for k in range(1, nx):
            src = lax.rem(me_x + k, nx)
            for c in range(2):
                ref = recv.at[src, pl.ds(c * half_rows, half_rows), pl.ds(local * W, W)]
                pltpu.make_async_remote_copy(
                    src_ref=ref, dst_ref=ref, send_sem=rs_s.at[0], recv_sem=rs_r.at[src, local, c], **device(sibling),
                ).wait_recv()


slot_kinds = "UUDUUDUUUDDDDD"
slot_pieces = (
    0xECA86420, 0xFDB97531,
    0xECA96420, 0xCA86420E,
    0xDB97531F, 0xCAB87501,
    0xA86420EC, 0xB97531FD,
    0x86420ECA, 0xAB87423E,
    0xB896501C, 0x897423EA,
    0x926501F0, 0xFD023EC0,
)
slot_live = (0xFF, 0xFF, 0xFF, 0xFF, 0xFF, 0xFF, 0xFF, 0xFF, 0xFF, 0xFF, 0xFF, 0xFF, 0xFE, 0xDE)
slot_ahead = (1, 2, 2, 2, 2, 2, 2, 2, 2, 2, 1, 1, 1, 2)
relays = ((1, 13), (4, 15), (7, 11))
relay_place = 6
ring_places = 8
last_chunks = 4
tiles_per_step = 3


def look(word, place, width):
    word = word - 2**32 if word >= 2**31 else word
    return lax.bitwise_and(lax.shift_right_logical(jnp.int32(word), place * width), jnp.int32(2**width - 1))


def routed_kernel(
    n_fs, n_tp, tokens, gain, up_l, dn_l, up_w, dn_w, recv, x, hid, part, stage, up_f, dn_f, gain_v, acc,
    loc_sem, tok_s, tok_r, ring_s, ring_r, y_s, y_r, pre_s, pre_r, rs_s, rs_r,
):
    nz, ny = grid_of(n_fs)
    me_f, me_t = lax.axis_index("fs"), lax.axis_index("tp")
    T, Dk = tokens.shape
    R, F = up_l.shape
    D = n_fs * R
    W = R // 2
    nx = n_tp // 2
    me_x, me_c = lax.div(me_t, 2), lax.rem(me_t, 2)
    sibling = me_t + 1 - 2 * me_c
    half_rows = T // 2
    per_owner = Dk // W
    S = len(slot_kinds)
    last = S - 1

    mz, my = lax.div(me_f, ny), lax.rem(me_f, ny)
    lane = mz + me_x * (nz - 1 - 2 * mz)
    pos = lane + my * (n_fs - 1 - 2 * lane)

    def at(p):
        side = lax.div(p, nz)
        along = p + side * (n_fs - 1 - 2 * p)
        return (along + me_x * (nz - 1 - 2 * along)) * ny + side

    right, left, across = at(lax.rem(pos + 1, n_fs)), at(lax.rem(pos + n_fs - 1, n_fs)), at(n_fs - 1 - pos)
    seat = (pos, n_fs - 1 - pos)
    behind = tuple(lax.rem(p + n_fs - 1, n_fs) for p in seat)
    is_relay = (pos == relay_place) | (pos == n_fs - 1 - relay_place)

    def tp_peer(k):
        return lax.rem(me_t + k, n_tp)

    barrier = pltpu.get_barrier_semaphore()
    for f in (right, left, across):
        pl.semaphore_signal(barrier, inc=1, device_id={"fs": f, "tp": me_t}, device_id_type=MESH)
    for k in range(1, n_tp):
        pl.semaphore_signal(barrier, inc=1, device_id={"fs": me_f, "tp": tp_peer(k)}, device_id_type=MESH)

    def tok_cols(t):
        return x.at[:, pl.ds(pl.multiple_of(t * Dk, Dk), Dk)]

    gain_copy = pltpu.make_async_copy(gain, gain_v, loc_sem.at[0])
    up_copies = [
        pltpu.make_async_copy(up_l.at[pl.ds(h * W, W), :], up_f.at[pl.ds(h * W, W), :], loc_sem.at[1 + h]) for h in range(2)
    ]
    tok_copy = pltpu.make_async_copy(tokens, tok_cols(me_t), loc_sem.at[3])
    dn_copy = pltpu.make_async_copy(dn_l, dn_f, loc_sem.at[4])
    for c in [gain_copy] + up_copies + [dn_copy, tok_copy]:
        c.start()

    def mirrored(code, m):
        src, half = lax.div(code, 2), lax.rem(code, 2)
        return at(src + m * (n_fs - 1 - 2 * src)), half + m * (1 - 2 * half)

    def piece(s, place, d):
        return mirrored(look(slot_pieces[s], place, 4), d)

    def live(s, place):
        return None if slot_live[s] == 2**n_fs - 1 else look(slot_live[s], place, 1) == 1

    def when(pred, body):
        if pred is None:
            body()
        else:
            pl.when(pred)(body)

    def chunks(s):
        return last_chunks if s == last else 2

    def index(s, c):
        return 2 * s + c

    def ref_of(kind, f, half, c, n):
        if kind == "U":
            rows = W // n
            return up_w.at[pl.ds(pl.multiple_of(f * R + half * W + c * rows, rows), rows), :]
        return dn_w.at[pl.ds(c * (F // n), F // n), pl.ds(pl.multiple_of(f * R + half * W, W), W)]

    def ring_copy(s, c, d, place):
        f, half = piece(s, place, d)
        ref = ref_of(slot_kinds[s], f, half, c, chunks(s))
        return pltpu.make_async_remote_copy(
            src_ref=ref, dst_ref=ref, send_sem=ring_s.at[d, index(s, c)], recv_sem=ring_r.at[d, index(s, c)],
            device_id={"fs": right if d == 0 else left, "tp": me_t}, device_id_type=MESH,
        )

    def send(s, c):
        for d in range(2):
            when(live(s, seat[d]), lambda: ring_copy(s, c, d, seat[d]).start())

    def arrive(s, c):
        for d in range(2):
            when(live(s, behind[d]), lambda: ring_copy(s, c, d, behind[d]).wait_recv())

    def relay_copy(j, m):
        f, half = mirrored(jnp.int32(relays[j][1]), m)
        ref = ref_of("D", f, half, 0, 1)
        return pltpu.make_async_remote_copy(
            src_ref=ref, dst_ref=ref, send_sem=y_s.at[j], recv_sem=y_r.at[j],
            device_id={"fs": across, "tp": me_t}, device_id_type=MESH,
        )

    relay_out = jnp.where(pos == relay_place, 0, 1)

    own_row = pl.multiple_of(me_f * R, R)
    gain_copy.wait()
    spread = jnp.transpose(jnp.broadcast_to(gain_v[...], (128, R)))
    for h in range(2):
        up_copies[h].wait()
        for c in range(F // 128):
            cols = pl.ds(c * 128, 128)
            up_w[pl.ds(own_row + h * W, W), cols] = (
                spread[h * W : (h + 1) * W] * up_f[pl.ds(h * W, W), cols]
            ).astype(jnp.bfloat16)
    pl.semaphore_wait(barrier, n_tp + 2)
    for t in range(2):
        if t < slot_ahead[t]:
            for e in range(2):
                send(t, e)

    def token_copy(k):
        return pltpu.make_async_remote_copy(
            src_ref=tok_cols(me_t), dst_ref=tok_cols(me_t), send_sem=tok_s.at[k], recv_sem=tok_r.at[k],
            device_id={"fs": me_f, "tp": tp_peer(k)}, device_id_type=MESH,
        )

    tok_copy.wait()
    for k in range(1, n_tp):
        token_copy(k).start()
    dn_copy.wait()
    block = min(F, 256)

    @pl.loop(0, F // block)
    def _(i):
        r = pl.ds(pl.multiple_of(i * block, block), block)
        dn_w[r, pl.ds(own_row, R)] = jnp.transpose(dn_f[:, r]).astype(jnp.bfloat16)

    def normalise():
        for k in range(1, n_tp):
            src = lax.rem(me_t - k + n_tp, n_tp)
            pltpu.make_async_remote_copy(
                src_ref=tok_cols(src), dst_ref=tok_cols(src), send_sem=tok_s.at[k], recv_sem=tok_r.at[k],
                device_id={"fs": me_f, "tp": tp_peer(k)}, device_id_type=MESH,
            ).wait_recv()
            token_copy(k).wait_send()
        rows = 64

        @pl.loop(0, T // rows)
        def _(i):
            r = pl.ds(pl.multiple_of(i * rows, rows), rows)
            v = x[r, :].astype(jnp.float32)
            x[r, :] = (v * lax.rsqrt(jnp.mean(v * v, axis=-1, keepdims=True) + norm_floor)).astype(jnp.bfloat16)

    width = 256

    def make_hidden(first, count):
        @pl.loop(first, first + count)
        def _(i):
            c = pl.ds(pl.multiple_of(i * width, width), width)
            pre = jnp.dot(x[...], up_w[:, c], preferred_element_type=jnp.float32)
            hid[:, c] = jnp.square(jnp.maximum(pre, 0.0)).astype(jnp.bfloat16)

    my_half = pl.ds(pl.multiple_of(me_c * half_rows, half_rows), half_rows)
    its_half = pl.ds(pl.multiple_of((1 - me_c) * half_rows, half_rows), half_rows)

    def device(t):
        return dict(device_id={"fs": me_f, "tp": t}, device_id_type=MESH)

    def cols_of(q):
        return pl.ds(pl.multiple_of(lax.rem(q, per_owner) * W, W), W)

    def tile(q):
        return pl.ds(pl.multiple_of(q * W, W), W)

    def whole_copy(q):
        return pltpu.make_async_remote_copy(
            src_ref=part.at[q], dst_ref=recv.at[nx, :, cols_of(q)],
            send_sem=rs_s.at[q], recv_sem=rs_r.at[nx, lax.rem(q, per_owner), 0], **device(sibling),
        )

    def pair_copy(q):
        return pltpu.make_async_remote_copy(
            src_ref=part.at[q, its_half], dst_ref=stage.at[q],
            send_sem=pre_s.at[q], recv_sem=pre_r.at[q], **device(sibling),
        )

    def half_copy(q):
        return pltpu.make_async_remote_copy(
            src_ref=part.at[q, my_half], dst_ref=recv.at[me_x, my_half, cols_of(q)],
            send_sem=rs_s.at[q], recv_sem=rs_r.at[me_x, lax.rem(q, per_owner), me_c],
            **device(lax.div(q, per_owner)),
        )

    def pass_on(q):
        @pl.when(lax.div(q, 2 * per_owner) != me_x)
        def _():
            pair_copy(q).wait_recv()
            both = part[q, my_half, :].astype(jnp.float32) + stage[q].astype(jnp.float32)
            part[q, my_half, :] = both.astype(jnp.bfloat16)
            half_copy(q).start()

    def do_part(q):
        owner = lax.div(q, per_owner)

        @pl.loop(0, 2)
        def _(i):
            r = pl.ds(pl.multiple_of(lax.rem(i + 1 + me_c, 2) * half_rows, half_rows), half_rows)
            part[q, r, :] = jnp.dot(hid[r, :], dn_w[:, tile(q)], preferred_element_type=jnp.float32).astype(jnp.bfloat16)

            @pl.when((i == 0) & (lax.div(owner, nx) != me_x))
            def _():
                pair_copy(q).start()

            @pl.when((i == 1) & (owner == sibling))
            def _():
                whole_copy(q).start()

    def entry_of(e):
        kind = e[0]
        if kind == "none":
            return jnp.int32(0), jnp.int32(0)
        if kind == "own":
            return me_f * 2 + e[1], jnp.int32(1)
        if kind == "relay":
            f, half = mirrored(jnp.int32(relays[e[1]][1]), 1 - relay_out)
            return f * 2 + half, jnp.where(is_relay, 1, 0)
        s, d = e[1], e[2]
        f, half = piece(s, behind[d], d)
        ok = jnp.int32(1) if slot_live[s] == 2**n_fs - 1 else look(slot_live[s], behind[d], 1)
        return f * 2 + half, ok

    def pick(i, values):
        out = values[0]
        for k in range(1, len(values)):
            out = jnp.where(i == k, values[k], out)
        return out

    def run_tiles(before, entries):
        cur = [entry_of(e) for e in entries]
        prev = [entry_of(before)] + cur[:-1]

        @pl.loop(0, len(entries))
        def _(i):
            q = pick(i, [v[0] for v in cur])

            @pl.when(pick(i, [v[1] for v in cur]) == 1)
            def _():
                do_part(q)

            p = pick(i, [v[0] for v in prev])

            @pl.when(pick(i, [v[1] for v in prev]) == 1)
            def _():
                pass_on(p)

    def tail_tiles(c):
        tiles = []
        for d in range(2):
            f, half = piece(last, behind[d], d)
            tiles.append(f * 2 + half)
        rows = half_rows
        k = pl.ds(c * (F // last_chunks), F // last_chunks)

        def body():
            both = jnp.concatenate([dn_w[k, tile(q)] for q in tiles], axis=1)

            @pl.loop(0, T // rows)
            def _(i):
                r = pl.ds(pl.multiple_of(i * rows, rows), rows)
                out = jnp.dot(hid[r, k], both, preferred_element_type=jnp.float32)
                if c > 0:
                    out += acc[r, :]
                if c < last_chunks - 1:
                    acc[r, :] = out
                else:
                    for j, q in enumerate(tiles):
                        part[q, r, :] = out[:, j * W : (j + 1) * W].astype(jnp.bfloat16)

            if c == last_chunks - 1:
                for q in tiles:
                    @pl.when(lax.div(q, per_owner) == sibling)
                    def _():
                        whole_copy(q).start()

        when(live(last, behind[0]), body)

    def send_after(t, e):
        if t == last:
            return (t - 1, 0)
        return (t - slot_ahead[t], e)

    queue = [("own", h) for h in range(2)]
    hidden_from = 2 * max(s for s in range(S) if slot_kinds[s] == "U") + 1
    blocks = F // width
    per_step = (blocks + 1) // 2
    prior = ("none",)
    normal_at = max(0, hidden_from - 6)

    for s in range(S):
        for c in range(chunks(s)):
            k = index(s, c)
            arrive(s, c)
            for j, (t, _) in enumerate(relays):
                if t + 1 == s and c == 0:
                    @pl.when(is_relay)
                    def _():
                        relay_copy(j, 1 - relay_out).wait_recv()
                    queue.append(("relay", j))
            for t in range(s + 1, S):
                for e in range(chunks(t)):
                    if send_after(t, e) == (s, c):
                        send(t, e)
            if c == 1 and s < last:
                for j, (t, _) in enumerate(relays):
                    if t == s + 1:
                        @pl.when(is_relay)
                        def _():
                            relay_copy(j, relay_out).start()
                if slot_kinds[s] == "D":
                    queue += [("ring", s, d) for d in range(2)]
            if k == normal_at:
                normalise()
            if k in (hidden_from, hidden_from + 1):
                make_hidden((k - hidden_from) * per_step, min(per_step, blocks - (k - hidden_from) * per_step))
            if k > hidden_from + 1 and (s, c) < (last - 1, 1) and queue:
                take = queue[:tiles_per_step]
                queue = queue[tiles_per_step:]
                run_tiles(prior, take)
                prior = take[-1]
            if (s, c) == (last - 1, 1):
                if queue:
                    run_tiles(prior, queue)
                    prior = queue[-1]
                    queue = []
                q, ok = entry_of(prior)

                @pl.when(ok == 1)
                def _():
                    pass_on(q)
            if s == last:
                tail_tiles(c)

    @pl.loop(0, per_owner)
    def _(local):
        cols = pl.ds(pl.multiple_of(local * W, W), W)
        recv[me_x, :, cols] = part[me_t * per_owner + local]

    for s in range(S):
        for c in range(chunks(s)):
            for d in range(2):
                when(live(s, seat[d]), lambda: ring_copy(s, c, d, seat[d]).wait_send())
    for j in range(len(relays)):
        @pl.when(is_relay)
        def _():
            relay_copy(j, relay_out).wait_send()

    @pl.loop(0, D // W)
    def _(q):
        owner = lax.div(q, per_owner)

        @pl.when(owner == sibling)
        def _():
            whole_copy(q).wait_send()

        @pl.when(lax.div(owner, nx) != me_x)
        def _():
            pair_copy(q).wait_send()
            half_copy(q).wait_send()

    for local in range(per_owner):
        q = me_t * per_owner + local
        whole_copy(q).wait_recv()
        for k in range(1, nx):
            src = lax.rem(me_x + k, nx)
            for c in range(2):
                ref = recv.at[src, pl.ds(c * half_rows, half_rows), pl.ds(local * W, W)]
                pltpu.make_async_remote_copy(
                    src_ref=ref, dst_ref=ref, send_sem=rs_s.at[0], recv_sem=rs_r.at[src, local, c], **device(sibling),
                ).wait_recv()


def finish_kernel(up_v, dn_v, recv, up_o, dn_o, mlp_o, total, sem):
    copies = [pltpu.make_async_copy(up_v, up_o, sem.at[0]), pltpu.make_async_copy(dn_v, dn_o, sem.at[1])]
    for c in copies:
        c.start()
    n, T, _ = recv.shape
    rows = 128

    @pl.loop(0, T // rows)
    def _(i):
        r = pl.ds(pl.multiple_of(i * rows, rows), rows)
        acc = recv[0, r, :].astype(jnp.float32)
        for k in range(1, n):
            acc += recv[k, r, :].astype(jnp.float32)
        total[r, :] = acc.astype(jnp.bfloat16)

    last = pltpu.make_async_copy(total, mlp_o, sem.at[2])
    last.start()
    for c in copies:
        c.wait()
    last.wait()


def solution(mesh):
    n_fs, n_tp = mesh.shape["fs"], mesh.shape["tp"]
    bf16 = jnp.bfloat16

    def on_device(tokens, norm_gain, up_master, down_master):
        T, Dk = tokens.shape
        R, F = up_master.shape
        D = n_fs * R
        W = R // 2 if (R // 2) % 128 == 0 else R
        S = len(send_list(n_fs))
        any_spec = pl.BlockSpec(memory_space=pl.ANY)
        vmem_spec = pl.BlockSpec(memory_space=pltpu.VMEM)
        routed = (n_fs, grid_of(n_fs)[1], n_tp * grid_of(n_fs)[1], 2 * W) == (ring_places, 2, n_fs, R)
        waves = 2 * len(slot_kinds) + last_chunks - 2 if routed else S
        own_sems = 5 if routed else 4
        extra = [pltpu.VMEM((T, 2 * W), jnp.float32)] if routed else []
        relay_sems = [pltpu.SemaphoreType.DMA((len(relays),))] * 2 if routed else []
        up_v, dn_v, recv = pl.pallas_call(
            functools.partial(routed_kernel if routed else gather_kernel, n_fs, n_tp),
            out_shape=(pltpu.VMEM((D, F), bf16), pltpu.VMEM((F, D), bf16), pltpu.VMEM((n_tp // 2 + 1, T, Dk), bf16)),
            in_specs=[pl.BlockSpec(memory_space=pltpu.HBM)] * 4,
            out_specs=(vmem_spec,) * 3,
            scratch_shapes=[
                pltpu.VMEM((T, D), bf16),
                pltpu.VMEM((T, F), bf16),
                pltpu.VMEM((D // W, T, W), bf16),
                pltpu.VMEM((D // W, T // 2, W), bf16),
                pltpu.VMEM((R, F), jnp.float32),
                pltpu.VMEM((R, F), jnp.float32),
                pltpu.VMEM((1, R), jnp.float32),
                *extra,
                pltpu.SemaphoreType.DMA((own_sems,)),
                pltpu.SemaphoreType.DMA((n_tp,)),
                pltpu.SemaphoreType.DMA((n_tp,)),
                pltpu.SemaphoreType.DMA((2, waves)),
                pltpu.SemaphoreType.DMA((2, waves)),
                *relay_sems,
                pltpu.SemaphoreType.DMA((D // W,)),
                pltpu.SemaphoreType.DMA((D // W,)),
                pltpu.SemaphoreType.DMA((D // W,)),
                pltpu.SemaphoreType.DMA((n_tp // 2 + 1, Dk // W, 2)),
            ],
            compiler_params=pltpu.CompilerParams(
                collective_id=0, has_side_effects=True, vmem_limit_bytes=44 * 2**20
            ),
        )(tokens, norm_gain[None, :], up_master, down_master)
        return pl.pallas_call(
            finish_kernel,
            out_shape=(
                jax.ShapeDtypeStruct((D, F), bf16),
                jax.ShapeDtypeStruct((F, D), bf16),
                jax.ShapeDtypeStruct((T, Dk), bf16),
            ),
            in_specs=[vmem_spec] * 3,
            out_specs=(any_spec,) * 3,
            scratch_shapes=[pltpu.VMEM((T, Dk), bf16), pltpu.SemaphoreType.DMA((3,))],
            compiler_params=pltpu.CompilerParams(vmem_limit_bytes=8 * 2**20),
        )(up_v, dn_v, recv)

    in_specs = (P("fs", "tp"), P("fs"), P("fs", "tp"), P("fs", "tp"))
    out_specs = (P(None, "tp"), P("tp", None), P("fs", "tp"))
    return jax.shard_map(on_device, mesh=mesh, in_specs=in_specs, out_specs=out_specs, check_vma=False)
```

```python
import functools

import jax
import jax.numpy as jnp
from jax import lax
from jax.experimental import pallas as pl
from jax.experimental.pallas import tpu as pltpu
from jax.sharding import PartitionSpec as P

norm_floor = 1e-06
MESH = pl.DeviceIdType.MESH


def grid_of(n):
    ny = max(d for d in range(1, n + 1) if n % d == 0 and d * d <= n)
    return n // ny, ny


def position_of(f, nz, ny):
    if ny == 1:
        return f
    z, y = lax.div(f, ny), lax.rem(f, ny)
    tail = lax.div(y + (ny - 1), ny)
    k = nz - 1 - z
    odd = lax.rem(k, 2)
    r = (1 - odd) * (y - 1) + odd * (ny - 1 - y)
    return (1 - tail) * z + tail * (nz + k * (ny - 1) + r)


def index_at(p, nz, ny):
    if ny == 1:
        return p
    tail = lax.div(lax.div(p, nz) + (ny - 2), ny - 1)
    q = tail * (p - nz)
    k = lax.div(q, ny - 1)
    r = lax.rem(q, ny - 1)
    odd = lax.rem(k, 2)
    z = (1 - tail) * p + tail * (nz - 1 - k)
    y = tail * ((1 - odd) * (1 + r) + odd * (ny - 1 - r))
    return z * ny + y


def send_list(n):
    hops = n // 2
    split = n % 2 == 0

    def pieces(a, h):
        return [(a, h, 0)] if split and h == hops - 1 else [(a, h, 0), (a, h, 1)]

    ups = [p for h in range(1, hops) for p in pieces("u", h)]
    downs = [p for h in range(1, hops) for p in pieces("d", h)]
    own_u, own_d = pieces("u", 0), pieces("d", 0)
    return own_u + own_d[:1] + ups + own_d[1:] + downs


def gather_kernel(
    n_fs, n_tp, tokens, gain, up_l, dn_l, up_w, dn_w, recv, x, hid, part, stage, up_f, dn_f, gain_v,
    loc_sem, tok_s, tok_r, ring_s, ring_r, pre_s, pre_r, rs_s, rs_r,
):
    nz, ny = grid_of(n_fs)
    me_f, me_t = lax.axis_index("fs"), lax.axis_index("tp")
    pos = position_of(me_f, nz, ny)
    T, Dk = tokens.shape
    R, F = up_l.shape
    D = n_fs * R
    split_cols = (R // 2) % 128 == 0
    W = R // 2 if split_cols else R

    def at(offset):
        return index_at(lax.rem(pos + offset + n_fs, n_fs), nz, ny)

    right, left = at(1), at(-1)

    def tp_peer(k):
        return lax.rem(me_t + k, n_tp)

    barrier = pltpu.get_barrier_semaphore()
    for f in (right, left):
        pl.semaphore_signal(barrier, inc=1, device_id={"fs": f, "tp": me_t}, device_id_type=MESH)
    for k in range(1, n_tp):
        pl.semaphore_signal(barrier, inc=1, device_id={"fs": me_f, "tp": tp_peer(k)}, device_id_type=MESH)

    def up_piece(f, h):
        return up_w.at[pl.ds(pl.multiple_of(f * R + h * (R // 2), R // 2), R // 2), :]

    def dn_piece(f, h):
        if split_cols:
            return dn_w.at[:, pl.ds(pl.multiple_of(f * R + h * (R // 2), R // 2), R // 2)]
        return dn_w.at[pl.ds(h * (F // 2), F // 2), pl.ds(pl.multiple_of(f * R, R), R)]

    def tok_cols(t):
        return x.at[:, pl.ds(pl.multiple_of(t * Dk, Dk), Dk)]

    own = [
        pltpu.make_async_copy(up_l, up_f, loc_sem.at[0]),
        pltpu.make_async_copy(tokens, tok_cols(me_t), loc_sem.at[1]),
        pltpu.make_async_copy(dn_l, dn_f, loc_sem.at[2]),
    ]
    gain_copy = pltpu.make_async_copy(gain, gain_v, loc_sem.at[3])
    for c in [gain_copy] + own:
        c.start()
    own_rows = pl.ds(pl.multiple_of(me_f * R, R), R)
    gain_copy.wait()
    spread = jnp.transpose(jnp.broadcast_to(gain_v[...], (128, R)))
    own[0].wait()
    for c in range(F // 128):
        cols = pl.ds(c * 128, 128)
        up_w[own_rows, cols] = (spread * up_f[:, cols]).astype(jnp.bfloat16)
    own[1].wait()
    pl.semaphore_wait(barrier, n_tp + 1)

    order = send_list(n_fs)
    S = len(order)

    def ring_copy(s, d):
        a, hop, second = order[s]
        half = second if d == 0 else 1 - second
        f = at(-hop if d == 0 else hop)
        ref = up_piece(f, half) if a == "u" else dn_piece(f, half)
        return pltpu.make_async_remote_copy(
            src_ref=ref, dst_ref=ref, send_sem=ring_s.at[d, s], recv_sem=ring_r.at[d, s],
            device_id={"fs": right if d == 0 else left, "tp": me_t}, device_id_type=MESH,
        )

    def arrival(s, d):
        a, hop, second = order[s]
        half = second if d == 0 else 1 - second
        f = at(-(hop + 1) if d == 0 else hop + 1)
        return f, half, (up_piece(f, half) if a == "u" else dn_piece(f, half))

    def wait_arrival(s, d):
        f, half, ref = arrival(s, d)
        pltpu.make_async_remote_copy(
            src_ref=ref, dst_ref=ref, send_sem=ring_s.at[d, s], recv_sem=ring_r.at[d, s],
            device_id={"fs": right if d == 0 else left, "tp": me_t}, device_id_type=MESH,
        ).wait_recv()

    needs = [-1 if hop == 0 else order.index((a, hop - 1, second)) for a, hop, second in order]
    issued = [0]

    def issue(upto):
        while issued[0] < S and needs[issued[0]] <= upto:
            if upto < 0 and issued[0] >= 3:
                break
            for d in range(2):
                ring_copy(issued[0], d).start()
            issued[0] += 1

    for s in range(2):
        for d in range(2):
            ring_copy(s, d).start()

    def token_copy(k):
        return pltpu.make_async_remote_copy(
            src_ref=tok_cols(me_t), dst_ref=tok_cols(me_t), send_sem=tok_s.at[k], recv_sem=tok_r.at[k],
            device_id={"fs": me_f, "tp": tp_peer(k)}, device_id_type=MESH,
        )

    for k in range(1, n_tp):
        token_copy(k).start()
    own[2].wait()
    block = min(F, 256)

    @pl.loop(0, F // block)
    def _(i):
        r = pl.ds(pl.multiple_of(i * block, block), block)
        dn_w[r, own_rows] = jnp.transpose(dn_f[:, r]).astype(jnp.bfloat16)

    issued[0] = 2
    issue(-1)

    def normalise():
        for k in range(1, n_tp):
            src = lax.rem(me_t - k + n_tp, n_tp)
            pltpu.make_async_remote_copy(
                src_ref=tok_cols(src), dst_ref=tok_cols(src), send_sem=tok_s.at[k], recv_sem=tok_r.at[k],
                device_id={"fs": me_f, "tp": tp_peer(k)}, device_id_type=MESH,
            ).wait_recv()
            token_copy(k).wait_send()
        rows = 64

        @pl.loop(0, T // rows)
        def _(i):
            r = pl.ds(pl.multiple_of(i * rows, rows), rows)
            v = x[r, :].astype(jnp.float32)
            x[r, :] = (v * lax.rsqrt(jnp.mean(v * v, axis=-1, keepdims=True) + norm_floor)).astype(jnp.bfloat16)

    def make_hidden():
        width = 256

        @pl.loop(0, F // width)
        def _(i):
            c = pl.ds(pl.multiple_of(i * width, width), width)
            pre = jnp.dot(x[...], up_w[:, c], preferred_element_type=jnp.float32)
            hid[:, c] = jnp.square(jnp.maximum(pre, 0.0)).astype(jnp.bfloat16)

    per_owner = Dk // W
    nx = n_tp // 2
    half_rows = T // 2
    me_x, me_c = lax.div(me_t, 2), lax.rem(me_t, 2)
    sibling = me_t + 1 - 2 * me_c
    my_half = pl.ds(pl.multiple_of(me_c * half_rows, half_rows), half_rows)
    its_half = pl.ds(pl.multiple_of((1 - me_c) * half_rows, half_rows), half_rows)

    def device(t):
        return dict(device_id={"fs": me_f, "tp": t}, device_id_type=MESH)

    def cols_of(q):
        return pl.ds(pl.multiple_of(lax.rem(q, per_owner) * W, W), W)

    def whole_copy(q):
        return pltpu.make_async_remote_copy(
            src_ref=part.at[q], dst_ref=recv.at[nx, :, cols_of(q)],
            send_sem=rs_s.at[q], recv_sem=rs_r.at[nx, lax.rem(q, per_owner), 0], **device(sibling),
        )

    def pair_copy(q):
        return pltpu.make_async_remote_copy(
            src_ref=part.at[q, its_half], dst_ref=stage.at[q],
            send_sem=pre_s.at[q], recv_sem=pre_r.at[q], **device(sibling),
        )

    def half_copy(q):
        return pltpu.make_async_remote_copy(
            src_ref=part.at[q, my_half], dst_ref=recv.at[me_x, my_half, cols_of(q)],
            send_sem=rs_s.at[q], recv_sem=rs_r.at[me_x, lax.rem(q, per_owner), me_c],
            **device(lax.div(q, per_owner)),
        )

    def pass_on(q):
        @pl.when(lax.div(q, 2 * per_owner) != me_x)
        def _():
            pair_copy(q).wait_recv()
            both = part[q, my_half, :].astype(jnp.float32) + stage[q].astype(jnp.float32)
            part[q, my_half, :] = both.astype(jnp.bfloat16)
            half_copy(q).start()

    def do_parts(first, count):
        c = pl.ds(pl.multiple_of(first * W, W), count * W)

        @pl.loop(0, 2)
        def _(i):
            r = pl.ds(pl.multiple_of(lax.rem(i + 1 + me_c, 2) * half_rows, half_rows), half_rows)
            out = jnp.dot(hid[r, :], dn_w[:, c], preferred_element_type=jnp.float32).astype(jnp.bfloat16)
            for k in range(count):
                part[first + k, r, :] = out[:, k * W : (k + 1) * W]
            for k in range(count):
                owner = lax.div(first + k, per_owner)

                @pl.when((i == 0) & (lax.div(owner, 2) != me_x))
                def _():
                    pair_copy(first + k).start()

                @pl.when((i == 1) & (owner == sibling))
                def _():
                    whole_copy(first + k).start()

    per_chunk = R // W
    ready = [(me_f * per_chunk, per_chunk)]
    last_up = max(s for s in range(S) if order[s][0] == "u")
    norm_at = max(0, last_up - 2)
    for s in range(S):
        for d in range(2):
            wait_arrival(s, d)
        issue(s)
        a, hop, _ = order[s]
        if a == "d" and split_cols:
            if n_fs % 2 == 0 and hop == n_fs // 2 - 1:
                ready.append((at(hop + 1) * 2, 2))
            else:
                for d in range(2):
                    f, half, _ = arrival(s, d)
                    ready.append((f * 2 + half, 1))
        if s == norm_at:
            normalise()
        if s == last_up:
            make_hidden()
        if s >= last_up:
            for first, count in ready:
                do_parts(first, count)
            for first, count in ready:
                for k in range(count):
                    pass_on(first + k)
            ready = []
    if not split_cols:
        @pl.loop(0, n_fs)
        def _(q):
            @pl.when(q != me_f)
            def _():
                do_parts(q, 1)
                pass_on(q)

    @pl.loop(0, per_owner)
    def _(local):
        cols = pl.ds(pl.multiple_of(local * W, W), W)
        recv[me_x, :, cols] = part[me_t * per_owner + local]

    for d in range(2):
        for s in range(S):
            ring_copy(s, d).wait_send()

    @pl.loop(0, D // W)
    def _(q):
        owner = lax.div(q, per_owner)

        @pl.when(owner == sibling)
        def _():
            whole_copy(q).wait_send()

        @pl.when(lax.div(owner, 2) != me_x)
        def _():
            pair_copy(q).wait_send()
            half_copy(q).wait_send()

    for local in range(per_owner):
        q = me_t * per_owner + local
        whole_copy(q).wait_recv()
        for k in range(1, nx):
            src = lax.rem(me_x + k, nx)
            for c in range(2):
                ref = recv.at[src, pl.ds(c * half_rows, half_rows), pl.ds(local * W, W)]
                pltpu.make_async_remote_copy(
                    src_ref=ref, dst_ref=ref, send_sem=rs_s.at[0], recv_sem=rs_r.at[src, local, c], **device(sibling),
                ).wait_recv()


def finish_kernel(up_v, dn_v, recv, up_o, dn_o, mlp_o, total, sem):
    copies = [pltpu.make_async_copy(up_v, up_o, sem.at[0]), pltpu.make_async_copy(dn_v, dn_o, sem.at[1])]
    for c in copies:
        c.start()
    n, T, _ = recv.shape
    rows = 128

    @pl.loop(0, T // rows)
    def _(i):
        r = pl.ds(pl.multiple_of(i * rows, rows), rows)
        acc = recv[0, r, :].astype(jnp.float32)
        for k in range(1, n):
            acc += recv[k, r, :].astype(jnp.float32)
        total[r, :] = acc.astype(jnp.bfloat16)

    last = pltpu.make_async_copy(total, mlp_o, sem.at[2])
    last.start()
    for c in copies:
        c.wait()
    last.wait()


slot_kinds = "UUDUUDUUUDDDDD"
slot_pieces = (
    0xECA86420, 0xFDB97531,
    0xECA96420, 0xCA86420E,
    0xDB97531F, 0xCAB87501,
    0xA86420EC, 0xB97531FD,
    0x86420ECA, 0xAB87423E,
    0xB896501C, 0x897423EA,
    0x926501F0, 0xFD023EC0,
)
slot_live = (0xFF, 0xFF, 0xFF, 0xFF, 0xFF, 0xFF, 0xFF, 0xFF, 0xFF, 0xFF, 0xFF, 0xFF, 0xFE, 0xDE)
slot_ahead = (1, 2, 2, 2, 2, 2, 2, 2, 2, 2, 1, 1, 1, 2)
relays = ((1, 13), (4, 15), (7, 11))
relay_place = 6
ring_places = 8
last_chunks = 4
second_leads = 0x84
pairs_per_step = 2


def look(word, place, width):
    word = word - 2**32 if word >= 2**31 else word
    return lax.bitwise_and(lax.shift_right_logical(jnp.int32(word), place * width), jnp.int32(2**width - 1))


class Places:
    def __init__(self, n_fs, n_tp):
        nz, ny = grid_of(n_fs)
        self.n, self.nz, self.ny = n_fs, nz, ny
        self.me_f, self.me_t = lax.axis_index("fs"), lax.axis_index("tp")
        self.me_x, self.me_c = lax.div(self.me_t, 2), lax.rem(self.me_t, 2)
        z, y = lax.div(self.me_f, ny), lax.rem(self.me_f, ny)
        along = z + self.me_x * (nz - 1 - 2 * z)
        self.pos = along + y * (n_fs - 1 - 2 * along)
        self.seat = (self.pos, n_fs - 1 - self.pos)
        self.behind = tuple(lax.rem(p + n_fs - 1, n_fs) for p in self.seat)

    def at(self, p):
        side = lax.div(p, self.nz)
        along = p + side * (self.n - 1 - 2 * p)
        return (along + self.me_x * (self.nz - 1 - 2 * along)) * self.ny + side

    def mirrored(self, code, m):
        src, half = lax.div(code, 2), lax.rem(code, 2)
        return self.at(src + m * (self.n - 1 - 2 * src)), half + m * (1 - 2 * half)

    def piece(self, s, place, d):
        return self.mirrored(look(slot_pieces[s], place, 4), d)

    def live(self, s, place):
        return None if slot_live[s] == 2**self.n - 1 else look(slot_live[s], place, 1) == 1

    def last_tiles(self, per_owner):
        last = len(slot_kinds) - 1
        tiles = []
        for d in range(2):
            f, half = self.piece(last, self.behind[d], d)
            tiles.append(f * 2 + half)
        return self.live(last, self.behind[0]), tiles, [lax.div(q, per_owner) == self.me_t for q in tiles]


def routed_kernel(
    n_fs, n_tp, tokens, gain, up_l, dn_l, up_w, dn_w, recv, hid, x, part, stage, up_f, dn_f, gain_v, acc,
    loc_sem, tok_s, tok_r, ring_s, ring_r, y_s, y_r, pre_s, pre_r, rs_s, rs_r,
):
    here = Places(n_fs, n_tp)
    me_f, me_t, me_x, me_c, pos, at = here.me_f, here.me_t, here.me_x, here.me_c, here.pos, here.at
    seat, behind, mirrored, piece, live = here.seat, here.behind, here.mirrored, here.piece, here.live
    T, Dk = tokens.shape
    R, F = up_l.shape
    D = n_fs * R
    W = R // 2
    nx = n_tp // 2
    sibling = me_t + 1 - 2 * me_c
    half_rows = T // 2
    per_owner = Dk // W
    S = len(slot_kinds)
    last = S - 1

    right, left, across = at(lax.rem(pos + 1, n_fs)), at(lax.rem(pos + n_fs - 1, n_fs)), at(n_fs - 1 - pos)
    is_relay = (pos == relay_place) | (pos == n_fs - 1 - relay_place)

    def tp_peer(k):
        return lax.rem(me_t + k, n_tp)

    barrier = pltpu.get_barrier_semaphore()
    for f in (right, left, across):
        pl.semaphore_signal(barrier, inc=1, device_id={"fs": f, "tp": me_t}, device_id_type=MESH)
    for k in range(1, n_tp):
        pl.semaphore_signal(barrier, inc=1, device_id={"fs": me_f, "tp": tp_peer(k)}, device_id_type=MESH)

    def tok_cols(t):
        return x.at[:, pl.ds(pl.multiple_of(t * Dk, Dk), Dk)]

    quarter = W // 2
    gain_copy = pltpu.make_async_copy(gain, gain_v, loc_sem.at[0])
    firsts = [(h, c) for c in range(2) for h in range(2)]

    def up_copy(h, c):
        rows = pl.ds(h * W + c * quarter, quarter)
        return pltpu.make_async_copy(up_l.at[rows, :], up_f.at[rows, :], loc_sem.at[1 + 2 * h + c])

    tok_copy = pltpu.make_async_copy(tokens, tok_cols(me_t), loc_sem.at[5])
    dn_copy = pltpu.make_async_copy(dn_l, dn_f, loc_sem.at[6])
    gain_copy.start()
    for h, c in firsts:
        up_copy(h, c).start()

    def when(pred, body):
        if pred is None:
            body()
        else:
            pl.when(pred)(body)

    def chunks(s):
        return last_chunks if s == last else 2

    def index(s, c):
        return 2 * s + c

    def ref_of(kind, f, half, c, n):
        if kind == "U":
            rows = W // n
            return up_w.at[pl.ds(pl.multiple_of(f * R + half * W + c * rows, rows), rows), :]
        return dn_w.at[pl.ds(c * (F // n), F // n), pl.ds(pl.multiple_of(f * R + half * W, W), W)]

    def ring_copy(s, c, d, place):
        f, half = piece(s, place, d)
        ref = ref_of(slot_kinds[s], f, half, c, chunks(s))
        return pltpu.make_async_remote_copy(
            src_ref=ref, dst_ref=ref, send_sem=ring_s.at[d, index(s, c)], recv_sem=ring_r.at[d, index(s, c)],
            device_id={"fs": right if d == 0 else left, "tp": me_t}, device_id_type=MESH,
        )

    def send(s, c, sides=(0, 1)):
        for d in sides:
            when(live(s, seat[d]), lambda: ring_copy(s, c, d, seat[d]).start())

    def arrive(s, c):
        for d in range(2):
            when(live(s, behind[d]), lambda: ring_copy(s, c, d, behind[d]).wait_recv())

    def relay_copy(j, m):
        f, half = mirrored(jnp.int32(relays[j][1]), m)
        ref = ref_of("D", f, half, 0, 1)
        return pltpu.make_async_remote_copy(
            src_ref=ref, dst_ref=ref, send_sem=y_s.at[j], recv_sem=y_r.at[j],
            device_id={"fs": across, "tp": me_t}, device_id_type=MESH,
        )

    relay_out = jnp.where(pos == relay_place, 0, 1)

    own_row = pl.multiple_of(me_f * R, R)
    early_core = jnp.where(me_c == me_x, 0, 1)
    leads = [look(second_leads, seat[d], 1) == early_core for d in range(2)]
    gain_copy.wait()
    spread = jnp.transpose(jnp.broadcast_to(gain_v[...], (128, R)))

    def convert(h, c):
        up_copy(h, c).wait()
        first = h * W + c * quarter
        for j in range(F // 128):
            cols = pl.ds(j * 128, 128)
            up_w[pl.ds(own_row + first, quarter), cols] = (
                spread[first : first + quarter] * up_f[pl.ds(first, quarter), cols]
            ).astype(jnp.bfloat16)

    for h, c in firsts:
        convert(h, c)
        if (h, c) == (0, 0):
            pl.semaphore_wait(barrier, n_tp + 2)
        pl.when(leads[h])(lambda: send(0, c, (h,)))
        if (h, c) == (1, 0):
            tok_copy.start()
            dn_copy.start()
    for d in range(2):
        @pl.when(leads[d])
        def _():
            for e in range(2):
                send(1, e, (d,))

    def token_copy(k):
        return pltpu.make_async_remote_copy(
            src_ref=tok_cols(me_t), dst_ref=tok_cols(me_t), send_sem=tok_s.at[k], recv_sem=tok_r.at[k],
            device_id={"fs": me_f, "tp": tp_peer(k)}, device_id_type=MESH,
        )

    tok_copy.wait()
    for k in range(1, n_tp):
        token_copy(k).start()
    dn_copy.wait()
    block = min(F, 256)

    @pl.loop(0, F // block)
    def _(i):
        r = pl.ds(pl.multiple_of(i * block, block), block)
        dn_w[r, pl.ds(own_row, R)] = jnp.transpose(dn_f[:, r]).astype(jnp.bfloat16)

    for d in range(2):
        @pl.when(jnp.logical_not(leads[d]))
        def _():
            for t in range(2):
                for e in range(2):
                    send(t, e, (d,))

    def normalise():
        for k in range(1, n_tp):
            src = lax.rem(me_t - k + n_tp, n_tp)
            pltpu.make_async_remote_copy(
                src_ref=tok_cols(src), dst_ref=tok_cols(src), send_sem=tok_s.at[k], recv_sem=tok_r.at[k],
                device_id={"fs": me_f, "tp": tp_peer(k)}, device_id_type=MESH,
            ).wait_recv()
            token_copy(k).wait_send()
        rows = 64

        @pl.loop(0, T // rows)
        def _(i):
            r = pl.ds(pl.multiple_of(i * rows, rows), rows)
            v = x[r, :].astype(jnp.float32)
            x[r, :] = (v * lax.rsqrt(jnp.mean(v * v, axis=-1, keepdims=True) + norm_floor)).astype(jnp.bfloat16)

    width = 256

    def make_hidden(first, count):
        @pl.loop(first, first + count)
        def _(i):
            c = pl.ds(pl.multiple_of(i * width, width), width)
            pre = jnp.dot(x[...], up_w[:, c], preferred_element_type=jnp.float32)
            hid[:, c] = jnp.square(jnp.maximum(pre, 0.0)).astype(jnp.bfloat16)

    my_half = pl.ds(pl.multiple_of(me_c * half_rows, half_rows), half_rows)
    its_half = pl.ds(pl.multiple_of((1 - me_c) * half_rows, half_rows), half_rows)

    def device(t):
        return dict(device_id={"fs": me_f, "tp": t}, device_id_type=MESH)

    def cols_of(q):
        return pl.ds(pl.multiple_of(lax.rem(q, per_owner) * W, W), W)

    def tile(q):
        return pl.ds(pl.multiple_of(q * W, W), W)

    def whole_copy(q):
        return pltpu.make_async_remote_copy(
            src_ref=part.at[q], dst_ref=recv.at[nx, :, cols_of(q)],
            send_sem=rs_s.at[q], recv_sem=rs_r.at[nx, lax.rem(q, per_owner), 0], **device(sibling),
        )

    def pair_copy(q):
        return pltpu.make_async_remote_copy(
            src_ref=part.at[q, its_half], dst_ref=stage.at[q],
            send_sem=pre_s.at[q], recv_sem=pre_r.at[q], **device(sibling),
        )

    def half_copy(q):
        return pltpu.make_async_remote_copy(
            src_ref=part.at[q, my_half], dst_ref=recv.at[me_x, my_half, cols_of(q)],
            send_sem=rs_s.at[q], recv_sem=rs_r.at[me_x, lax.rem(q, per_owner), me_c],
            **device(lax.div(q, per_owner)),
        )

    def pass_on(q):
        @pl.when(lax.div(q, 2 * per_owner) != me_x)
        def _():
            pair_copy(q).wait_recv()
            both = part[q, my_half, :].astype(jnp.float32) + stage[q].astype(jnp.float32)
            part[q, my_half, :] = both.astype(jnp.bfloat16)
            half_copy(q).start()

    def do_pair(q, ok):
        use = [jnp.where(ok[0] == 1, q[0], q[1]), jnp.where(ok[1] == 1, q[1], q[0])]

        @pl.loop(0, 2)
        def _(i):
            r = pl.ds(pl.multiple_of(lax.rem(i + 1 + me_c, 2) * half_rows, half_rows), half_rows)
            both = jnp.concatenate([dn_w[:, tile(u)] for u in use], axis=1)
            out = jnp.dot(hid[r, :], both, preferred_element_type=jnp.float32).astype(jnp.bfloat16)
            for j in range(2):
                owner = lax.div(q[j], per_owner)

                @pl.when(ok[j] == 1)
                def _():
                    part[q[j], r, :] = out[:, j * W : (j + 1) * W]

                    @pl.when((i == 0) & (lax.div(owner, nx) != me_x))
                    def _():
                        pair_copy(q[j]).start()

                    @pl.when((i == 1) & (owner == sibling))
                    def _():
                        whole_copy(q[j]).start()

    def entry_of(e):
        kind = e[0]
        if kind == "none":
            return jnp.int32(0), jnp.int32(0)
        if kind == "own":
            return me_f * 2 + e[1], jnp.int32(1)
        if kind == "relay":
            f, half = mirrored(jnp.int32(relays[e[1]][1]), 1 - relay_out)
            return f * 2 + half, jnp.where(is_relay, 1, 0)
        s, d = e[1], e[2]
        f, half = piece(s, behind[d], d)
        ok = jnp.int32(1) if slot_live[s] == 2**n_fs - 1 else look(slot_live[s], behind[d], 1)
        return f * 2 + half, ok

    def pick(i, values):
        out = values[0]
        for k in range(1, len(values)):
            out = jnp.where(i == k, values[k], out)
        return out

    def pass_pair(q, ok):
        for j in range(2):
            @pl.when(ok[j] == 1)
            def _():
                pass_on(q[j])

    def run_tiles(before, pairs):
        cur = [[entry_of(e) for e in pair] for pair in pairs]
        prev = [[entry_of(e) for e in before]] + cur[:-1]

        @pl.loop(0, len(pairs))
        def _(i):
            def chosen(table, j, what):
                return pick(i, [pair[j][what] for pair in table])

            q, ok = [[chosen(cur, j, what) for j in range(2)] for what in range(2)]

            @pl.when(ok[0] + ok[1] > 0)
            def _():
                do_pair(q, ok)

            pass_pair(*[[chosen(prev, j, what) for j in range(2)] for what in range(2)])

    tail_on, tail_q, tail_mine = here.last_tiles(per_owner)
    depth = F // last_chunks

    def last_slot():
        theirs = [tail_on & jnp.logical_not(m) for m in tail_mine]
        for c in range(last_chunks):
            k = pl.ds(c * depth, depth)
            if c == 2:
                settle()
            for d in range(2):
                @pl.when(theirs[d])
                def _():
                    q = tail_q[d]
                    ring_copy(last, c, d, behind[d]).wait_recv()

                    @pl.loop(0, 2)
                    def _(i):
                        r = pl.ds(pl.multiple_of(i * half_rows, half_rows), half_rows)
                        out = jnp.dot(hid[r, k], dn_w[k, tile(q)], preferred_element_type=jnp.float32)
                        if c > 0:
                            out += acc[d, r, :]
                        if c < last_chunks - 1:
                            acc[d, r, :] = out
                        else:
                            part[q, r, :] = out.astype(jnp.bfloat16)

                    if c == last_chunks - 1:
                        whole_copy(q).start()

        for d in range(2):
            @pl.when(tail_on & tail_mine[d])
            def _():
                for c in range(last_chunks):
                    ring_copy(last, c, d, behind[d]).wait_recv()

    def in_tail(q):
        return tail_on & ((q == tail_q[0]) | (q == tail_q[1]))

    def settle():
        @pl.loop(0, per_owner)
        def _(local):
            q = me_t * per_owner + local

            @pl.when(jnp.logical_not(in_tail(q)))
            def _():
                recv[me_x, :, cols_of(q)] = part[q]
                whole_copy(q).wait_recv()

            @pl.when(in_tail(q))
            def _():
                recv[me_x, :, cols_of(q)] = jnp.zeros((T, W), jnp.bfloat16)

        for local in range(per_owner):
            for k in range(1, nx):
                src = lax.rem(me_x + k, nx)
                for c in range(2):
                    ref = recv.at[src, pl.ds(c * half_rows, half_rows), pl.ds(local * W, W)]
                    pltpu.make_async_remote_copy(
                        src_ref=ref, dst_ref=ref, send_sem=rs_s.at[0], recv_sem=rs_r.at[src, local, c], **device(sibling),
                    ).wait_recv()

        @pl.loop(0, D // W)
        def _(q):
            owner = lax.div(q, per_owner)

            @pl.when((owner == sibling) & jnp.logical_not(in_tail(q)))
            def _():
                whole_copy(q).wait_send()

            @pl.when(lax.div(owner, nx) != me_x)
            def _():
                pair_copy(q).wait_send()
                half_copy(q).wait_send()

        for j in range(len(relays)):
            @pl.when(is_relay)
            def _():
                relay_copy(j, relay_out).wait_send()

    def wait_sends(slots):
        for s in slots:
            for c in range(chunks(s)):
                for d in range(2):
                    when(live(s, seat[d]), lambda: ring_copy(s, c, d, seat[d]).wait_send())

    def send_after(t, e):
        if t == last:
            return (t - 1, 0)
        return (t - slot_ahead[t], e)

    queue = [[("own", h) for h in range(2)]]
    hidden_from = 2 * max(s for s in range(S) if slot_kinds[s] == "U") + 1
    blocks = F // width
    per_step = (blocks + 1) // 2
    prior = [("none",)] * 2
    normal_at = max(0, hidden_from - 6)

    for s in range(S):
        for c in range(chunks(s)):
            k = index(s, c)
            if s == last:
                if c == 0:
                    wait_sends(range(last - 2))
                    last_slot()
                continue
            arrive(s, c)
            for j, (t, _) in enumerate(relays):
                if t + 1 == s and c == 0:
                    @pl.when(is_relay)
                    def _():
                        relay_copy(j, 1 - relay_out).wait_recv()
                    if j % 2 == 0:
                        queue.append([("relay", j), ("none",)])
                    elif queue and queue[-1][0] == ("relay", j - 1):
                        queue[-1][1] = ("relay", j)
                    else:
                        queue.append([("relay", j), ("none",)])
            for t in range(s + 1, S):
                for e in range(chunks(t)):
                    if send_after(t, e) == (s, c):
                        send(t, e)
            if c == 1 and s < last:
                for j, (t, _) in enumerate(relays):
                    if t == s + 1:
                        @pl.when(is_relay)
                        def _():
                            relay_copy(j, relay_out).start()
                if slot_kinds[s] == "D":
                    queue.append([("ring", s, d) for d in range(2)])
            if k == normal_at:
                normalise()
            if k in (hidden_from, hidden_from + 1):
                make_hidden((k - hidden_from) * per_step, min(per_step, blocks - (k - hidden_from) * per_step))
            if k > hidden_from + 1 and queue:
                count = len(queue) if (s, c) == (last - 1, 1) else pairs_per_step
                take, queue = queue[:count], queue[count:]
                run_tiles(prior, take)
                prior = take[-1]
                if not queue:
                    final = [entry_of(e) for e in prior]
                    pass_pair([e[0] for e in final], [e[1] for e in final])
                    prior = [("none",)] * 2

    wait_sends(range(last - 2, S))
    for d in range(2):
        @pl.when(tail_on & (lax.div(tail_q[d], per_owner) == sibling))
        def _():
            whole_copy(tail_q[d]).wait_send()

        @pl.when(tail_on & tail_mine[d])
        def _():
            whole_copy(tail_q[d]).wait_recv()


def routed_finish(n_fs, n_tp, up_v, dn_v, recv, hid, up_o, dn_o, mlp_o, total, out, sem):
    here = Places(n_fs, n_tp)
    n, T, Dk = recv.shape
    W = up_v.shape[0] // n_fs // 2
    per_owner = Dk // W
    copies = []
    for k, (v, o) in enumerate(((up_v, up_o), (dn_v, dn_o))):
        half = v.shape[0] // 2
        copies += [
            pltpu.make_async_copy(v.at[pl.ds(h * half, half), :], o.at[pl.ds(h * half, half), :], sem.at[2 * k + h])
            for h in range(2)
        ]
    for c in copies:
        c.start()
    tail_on, tail_q, tail_mine = here.last_tiles(per_owner)
    rows = 128

    @pl.loop(0, T // rows)
    def _(i):
        r = pl.ds(pl.multiple_of(i * rows, rows), rows)
        acc = recv[0, r, :].astype(jnp.float32)
        for k in range(1, n):
            acc += recv[k, r, :].astype(jnp.float32)
        total[r, :] = acc

    for d in range(2):
        @pl.when(tail_on & tail_mine[d])
        def _():
            q = tail_q[d]
            cols = pl.ds(pl.multiple_of(lax.rem(q, per_owner) * W, W), W)
            own = dn_v.at[:, pl.ds(pl.multiple_of(q * W, W), W)]

            @pl.loop(0, 2)
            def _(i):
                r = pl.ds(pl.multiple_of(i * (T // 2), T // 2), T // 2)
                last = jnp.dot(hid[r, :], own[...], preferred_element_type=jnp.float32).astype(jnp.bfloat16)
                total[r, cols] += last.astype(jnp.float32)

    @pl.loop(0, T // rows)
    def _(i):
        r = pl.ds(pl.multiple_of(i * rows, rows), rows)
        out[r, :] = total[r, :].astype(jnp.bfloat16)

    written = pltpu.make_async_copy(out, mlp_o, sem.at[4])
    written.start()
    for c in copies:
        c.wait()
    written.wait()


def solution(mesh):
    n_fs, n_tp = mesh.shape["fs"], mesh.shape["tp"]
    bf16 = jnp.bfloat16

    def routed(tokens, norm_gain, up_master, down_master):
        T, Dk = tokens.shape
        R, F = up_master.shape
        D, W = n_fs * R, R // 2
        waves = 2 * len(slot_kinds) + last_chunks - 2
        hbm_spec = pl.BlockSpec(memory_space=pltpu.HBM)
        vmem_spec = pl.BlockSpec(memory_space=pltpu.VMEM)
        dma = pltpu.SemaphoreType.DMA
        held = pl.pallas_call(
            functools.partial(routed_kernel, n_fs, n_tp),
            out_shape=(
                pltpu.VMEM((D, F), bf16),
                pltpu.VMEM((F, D), bf16),
                pltpu.VMEM((n_tp // 2 + 1, T, Dk), bf16),
                pltpu.VMEM((T, F), bf16),
            ),
            in_specs=[hbm_spec] * 4,
            out_specs=(vmem_spec,) * 4,
            scratch_shapes=[
                pltpu.VMEM((T, D), bf16),
                pltpu.VMEM((D // W, T, W), bf16),
                pltpu.VMEM((D // W, T // 2, W), bf16),
                pltpu.VMEM((R, F), jnp.float32),
                pltpu.VMEM((R, F), jnp.float32),
                pltpu.VMEM((1, R), jnp.float32),
                pltpu.VMEM((2, T, W), jnp.float32),
                dma((7,)),
                dma((n_tp,)),
                dma((n_tp,)),
                dma((2, waves)),
                dma((2, waves)),
                dma((len(relays),)),
                dma((len(relays),)),
                dma((D // W,)),
                dma((D // W,)),
                dma((D // W,)),
                dma((n_tp // 2 + 1, Dk // W, 2)),
            ],
            compiler_params=pltpu.CompilerParams(
                collective_id=0, has_side_effects=True, vmem_limit_bytes=40 * 2**20
            ),
        )(tokens, norm_gain[None, :], up_master, down_master)
        return pl.pallas_call(
            functools.partial(routed_finish, n_fs, n_tp),
            out_shape=(
                jax.ShapeDtypeStruct((D, F), bf16),
                jax.ShapeDtypeStruct((F, D), bf16),
                jax.ShapeDtypeStruct((T, Dk), bf16),
            ),
            in_specs=[vmem_spec] * 4,
            out_specs=(pl.BlockSpec(memory_space=pl.ANY),) * 3,
            scratch_shapes=[pltpu.VMEM((T, Dk), jnp.float32), pltpu.VMEM((T, Dk), bf16), dma((5,))],
            compiler_params=pltpu.CompilerParams(vmem_limit_bytes=12 * 2**20),
        )(*held)

    def on_device(tokens, norm_gain, up_master, down_master):
        T, Dk = tokens.shape
        R, F = up_master.shape
        D = n_fs * R
        W = R // 2 if (R // 2) % 128 == 0 else R
        S = len(send_list(n_fs))
        any_spec = pl.BlockSpec(memory_space=pl.ANY)
        vmem_spec = pl.BlockSpec(memory_space=pltpu.VMEM)
        if (n_fs, grid_of(n_fs)[1], n_tp * grid_of(n_fs)[1], 2 * W) == (ring_places, 2, n_fs, R):
            return routed(tokens, norm_gain, up_master, down_master)
        up_v, dn_v, recv = pl.pallas_call(
            functools.partial(gather_kernel, n_fs, n_tp),
            out_shape=(pltpu.VMEM((D, F), bf16), pltpu.VMEM((F, D), bf16), pltpu.VMEM((n_tp // 2 + 1, T, Dk), bf16)),
            in_specs=[pl.BlockSpec(memory_space=pltpu.HBM)] * 4,
            out_specs=(vmem_spec,) * 3,
            scratch_shapes=[
                pltpu.VMEM((T, D), bf16),
                pltpu.VMEM((T, F), bf16),
                pltpu.VMEM((D // W, T, W), bf16),
                pltpu.VMEM((D // W, T // 2, W), bf16),
                pltpu.VMEM((R, F), jnp.float32),
                pltpu.VMEM((R, F), jnp.float32),
                pltpu.VMEM((1, R), jnp.float32),
                pltpu.SemaphoreType.DMA((4,)),
                pltpu.SemaphoreType.DMA((n_tp,)),
                pltpu.SemaphoreType.DMA((n_tp,)),
                pltpu.SemaphoreType.DMA((2, S)),
                pltpu.SemaphoreType.DMA((2, S)),
                pltpu.SemaphoreType.DMA((D // W,)),
                pltpu.SemaphoreType.DMA((D // W,)),
                pltpu.SemaphoreType.DMA((D // W,)),
                pltpu.SemaphoreType.DMA((n_tp // 2 + 1, Dk // W, 2)),
            ],
            compiler_params=pltpu.CompilerParams(
                collective_id=0, has_side_effects=True, vmem_limit_bytes=44 * 2**20
            ),
        )(tokens, norm_gain[None, :], up_master, down_master)
        return pl.pallas_call(
            finish_kernel,
            out_shape=(
                jax.ShapeDtypeStruct((D, F), bf16),
                jax.ShapeDtypeStruct((F, D), bf16),
                jax.ShapeDtypeStruct((T, Dk), bf16),
            ),
            in_specs=[vmem_spec] * 3,
            out_specs=(any_spec,) * 3,
            scratch_shapes=[pltpu.VMEM((T, Dk), bf16), pltpu.SemaphoreType.DMA((3,))],
            compiler_params=pltpu.CompilerParams(vmem_limit_bytes=8 * 2**20),
        )(up_v, dn_v, recv)

    in_specs = (P("fs", "tp"), P("fs"), P("fs", "tp"), P("fs", "tp"))
    out_specs = (P(None, "tp"), P("tp", None), P("fs", "tp"))
    return jax.shard_map(on_device, mesh=mesh, in_specs=in_specs, out_specs=out_specs, check_vma=False)
```

```python
import functools

import jax
import jax.numpy as jnp
from jax import lax
from jax.experimental import pallas as pl
from jax.experimental.pallas import tpu as pltpu
from jax.sharding import PartitionSpec as P

norm_floor = 1e-06
MESH = pl.DeviceIdType.MESH


def grid_of(n):
    ny = max(d for d in range(1, n + 1) if n % d == 0 and d * d <= n)
    return n // ny, ny


def position_of(f, nz, ny):
    if ny == 1:
        return f
    z, y = lax.div(f, ny), lax.rem(f, ny)
    tail = lax.div(y + (ny - 1), ny)
    k = nz - 1 - z
    odd = lax.rem(k, 2)
    r = (1 - odd) * (y - 1) + odd * (ny - 1 - y)
    return (1 - tail) * z + tail * (nz + k * (ny - 1) + r)


def index_at(p, nz, ny):
    if ny == 1:
        return p
    tail = lax.div(lax.div(p, nz) + (ny - 2), ny - 1)
    q = tail * (p - nz)
    k = lax.div(q, ny - 1)
    r = lax.rem(q, ny - 1)
    odd = lax.rem(k, 2)
    z = (1 - tail) * p + tail * (nz - 1 - k)
    y = tail * ((1 - odd) * (1 + r) + odd * (ny - 1 - r))
    return z * ny + y


def send_list(n):
    hops = n // 2
    split = n % 2 == 0

    def pieces(a, h):
        return [(a, h, 0)] if split and h == hops - 1 else [(a, h, 0), (a, h, 1)]

    ups = [p for h in range(1, hops) for p in pieces("u", h)]
    downs = [p for h in range(1, hops) for p in pieces("d", h)]
    own_u, own_d = pieces("u", 0), pieces("d", 0)
    return own_u + own_d[:1] + ups + own_d[1:] + downs


def gather_kernel(
    n_fs, n_tp, tokens, gain, up_l, dn_l, up_w, dn_w, recv, x, hid, part, stage, up_f, dn_f, gain_v,
    loc_sem, tok_s, tok_r, ring_s, ring_r, pre_s, pre_r, rs_s, rs_r,
):
    nz, ny = grid_of(n_fs)
    me_f, me_t = lax.axis_index("fs"), lax.axis_index("tp")
    pos = position_of(me_f, nz, ny)
    T, Dk = tokens.shape
    R, F = up_l.shape
    D = n_fs * R
    split_cols = (R // 2) % 128 == 0
    W = R // 2 if split_cols else R

    def at(offset):
        return index_at(lax.rem(pos + offset + n_fs, n_fs), nz, ny)

    right, left = at(1), at(-1)

    def tp_peer(k):
        return lax.rem(me_t + k, n_tp)

    barrier = pltpu.get_barrier_semaphore()
    for f in (right, left):
        pl.semaphore_signal(barrier, inc=1, device_id={"fs": f, "tp": me_t}, device_id_type=MESH)
    for k in range(1, n_tp):
        pl.semaphore_signal(barrier, inc=1, device_id={"fs": me_f, "tp": tp_peer(k)}, device_id_type=MESH)

    def up_piece(f, h):
        return up_w.at[pl.ds(pl.multiple_of(f * R + h * (R // 2), R // 2), R // 2), :]

    def dn_piece(f, h):
        if split_cols:
            return dn_w.at[:, pl.ds(pl.multiple_of(f * R + h * (R // 2), R // 2), R // 2)]
        return dn_w.at[pl.ds(h * (F // 2), F // 2), pl.ds(pl.multiple_of(f * R, R), R)]

    def tok_cols(t):
        return x.at[:, pl.ds(pl.multiple_of(t * Dk, Dk), Dk)]

    own = [
        pltpu.make_async_copy(up_l, up_f, loc_sem.at[0]),
        pltpu.make_async_copy(tokens, tok_cols(me_t), loc_sem.at[1]),
        pltpu.make_async_copy(dn_l, dn_f, loc_sem.at[2]),
    ]
    gain_copy = pltpu.make_async_copy(gain, gain_v, loc_sem.at[3])
    for c in [gain_copy] + own:
        c.start()
    own_rows = pl.ds(pl.multiple_of(me_f * R, R), R)
    gain_copy.wait()
    spread = jnp.transpose(jnp.broadcast_to(gain_v[...], (128, R)))
    own[0].wait()
    for c in range(F // 128):
        cols = pl.ds(c * 128, 128)
        up_w[own_rows, cols] = (spread * up_f[:, cols]).astype(jnp.bfloat16)
    own[1].wait()
    pl.semaphore_wait(barrier, n_tp + 1)

    order = send_list(n_fs)
    S = len(order)

    def ring_copy(s, d):
        a, hop, second = order[s]
        half = second if d == 0 else 1 - second
        f = at(-hop if d == 0 else hop)
        ref = up_piece(f, half) if a == "u" else dn_piece(f, half)
        return pltpu.make_async_remote_copy(
            src_ref=ref, dst_ref=ref, send_sem=ring_s.at[d, s], recv_sem=ring_r.at[d, s],
            device_id={"fs": right if d == 0 else left, "tp": me_t}, device_id_type=MESH,
        )

    def arrival(s, d):
        a, hop, second = order[s]
        half = second if d == 0 else 1 - second
        f = at(-(hop + 1) if d == 0 else hop + 1)
        return f, half, (up_piece(f, half) if a == "u" else dn_piece(f, half))

    def wait_arrival(s, d):
        f, half, ref = arrival(s, d)
        pltpu.make_async_remote_copy(
            src_ref=ref, dst_ref=ref, send_sem=ring_s.at[d, s], recv_sem=ring_r.at[d, s],
            device_id={"fs": right if d == 0 else left, "tp": me_t}, device_id_type=MESH,
        ).wait_recv()

    needs = [-1 if hop == 0 else order.index((a, hop - 1, second)) for a, hop, second in order]
    issued = [0]

    def issue(upto):
        while issued[0] < S and needs[issued[0]] <= upto:
            if upto < 0 and issued[0] >= 3:
                break
            for d in range(2):
                ring_copy(issued[0], d).start()
            issued[0] += 1

    for s in range(2):
        for d in range(2):
            ring_copy(s, d).start()

    def token_copy(k):
        return pltpu.make_async_remote_copy(
            src_ref=tok_cols(me_t), dst_ref=tok_cols(me_t), send_sem=tok_s.at[k], recv_sem=tok_r.at[k],
            device_id={"fs": me_f, "tp": tp_peer(k)}, device_id_type=MESH,
        )

    for k in range(1, n_tp):
        token_copy(k).start()
    own[2].wait()
    block = min(F, 256)

    @pl.loop(0, F // block)
    def _(i):
        r = pl.ds(pl.multiple_of(i * block, block), block)
        dn_w[r, own_rows] = jnp.transpose(dn_f[:, r]).astype(jnp.bfloat16)

    issued[0] = 2
    issue(-1)

    def normalise():
        for k in range(1, n_tp):
            src = lax.rem(me_t - k + n_tp, n_tp)
            pltpu.make_async_remote_copy(
                src_ref=tok_cols(src), dst_ref=tok_cols(src), send_sem=tok_s.at[k], recv_sem=tok_r.at[k],
                device_id={"fs": me_f, "tp": tp_peer(k)}, device_id_type=MESH,
            ).wait_recv()
            token_copy(k).wait_send()
        rows = 64

        @pl.loop(0, T // rows)
        def _(i):
            r = pl.ds(pl.multiple_of(i * rows, rows), rows)
            v = x[r, :].astype(jnp.float32)
            x[r, :] = (v * lax.rsqrt(jnp.mean(v * v, axis=-1, keepdims=True) + norm_floor)).astype(jnp.bfloat16)

    def make_hidden():
        width = 256

        @pl.loop(0, F // width)
        def _(i):
            c = pl.ds(pl.multiple_of(i * width, width), width)
            pre = jnp.dot(x[...], up_w[:, c], preferred_element_type=jnp.float32)
            hid[:, c] = jnp.square(jnp.maximum(pre, 0.0)).astype(jnp.bfloat16)

    per_owner = Dk // W
    nx = n_tp // 2
    half_rows = T // 2
    me_x, me_c = lax.div(me_t, 2), lax.rem(me_t, 2)
    sibling = me_t + 1 - 2 * me_c
    my_half = pl.ds(pl.multiple_of(me_c * half_rows, half_rows), half_rows)
    its_half = pl.ds(pl.multiple_of((1 - me_c) * half_rows, half_rows), half_rows)

    def device(t):
        return dict(device_id={"fs": me_f, "tp": t}, device_id_type=MESH)

    def cols_of(q):
        return pl.ds(pl.multiple_of(lax.rem(q, per_owner) * W, W), W)

    def whole_copy(q):
        return pltpu.make_async_remote_copy(
            src_ref=part.at[q], dst_ref=recv.at[nx, :, cols_of(q)],
            send_sem=rs_s.at[q], recv_sem=rs_r.at[nx, lax.rem(q, per_owner), 0], **device(sibling),
        )

    def pair_copy(q):
        return pltpu.make_async_remote_copy(
            src_ref=part.at[q, its_half], dst_ref=stage.at[q],
            send_sem=pre_s.at[q], recv_sem=pre_r.at[q], **device(sibling),
        )

    def half_copy(q):
        return pltpu.make_async_remote_copy(
            src_ref=part.at[q, my_half], dst_ref=recv.at[me_x, my_half, cols_of(q)],
            send_sem=rs_s.at[q], recv_sem=rs_r.at[me_x, lax.rem(q, per_owner), me_c],
            **device(lax.div(q, per_owner)),
        )

    def pass_on(q):
        @pl.when(lax.div(q, 2 * per_owner) != me_x)
        def _():
            pair_copy(q).wait_recv()
            both = part[q, my_half, :].astype(jnp.float32) + stage[q].astype(jnp.float32)
            part[q, my_half, :] = both.astype(jnp.bfloat16)
            half_copy(q).start()

    def do_parts(first, count):
        c = pl.ds(pl.multiple_of(first * W, W), count * W)

        @pl.loop(0, 2)
        def _(i):
            r = pl.ds(pl.multiple_of(lax.rem(i + 1 + me_c, 2) * half_rows, half_rows), half_rows)
            out = jnp.dot(hid[r, :], dn_w[:, c], preferred_element_type=jnp.float32).astype(jnp.bfloat16)
            for k in range(count):
                part[first + k, r, :] = out[:, k * W : (k + 1) * W]
            for k in range(count):
                owner = lax.div(first + k, per_owner)

                @pl.when((i == 0) & (lax.div(owner, 2) != me_x))
                def _():
                    pair_copy(first + k).start()

                @pl.when((i == 1) & (owner == sibling))
                def _():
                    whole_copy(first + k).start()

    per_chunk = R // W
    ready = [(me_f * per_chunk, per_chunk)]
    last_up = max(s for s in range(S) if order[s][0] == "u")
    norm_at = max(0, last_up - 2)
    for s in range(S):
        for d in range(2):
            wait_arrival(s, d)
        issue(s)
        a, hop, _ = order[s]
        if a == "d" and split_cols:
            if n_fs % 2 == 0 and hop == n_fs // 2 - 1:
                ready.append((at(hop + 1) * 2, 2))
            else:
                for d in range(2):
                    f, half, _ = arrival(s, d)
                    ready.append((f * 2 + half, 1))
        if s == norm_at:
            normalise()
        if s == last_up:
            make_hidden()
        if s >= last_up:
            for first, count in ready:
                do_parts(first, count)
            for first, count in ready:
                for k in range(count):
                    pass_on(first + k)
            ready = []
    if not split_cols:
        @pl.loop(0, n_fs)
        def _(q):
            @pl.when(q != me_f)
            def _():
                do_parts(q, 1)
                pass_on(q)

    @pl.loop(0, per_owner)
    def _(local):
        cols = pl.ds(pl.multiple_of(local * W, W), W)
        recv[me_x, :, cols] = part[me_t * per_owner + local]

    for d in range(2):
        for s in range(S):
            ring_copy(s, d).wait_send()

    @pl.loop(0, D // W)
    def _(q):
        owner = lax.div(q, per_owner)

        @pl.when(owner == sibling)
        def _():
            whole_copy(q).wait_send()

        @pl.when(lax.div(owner, 2) != me_x)
        def _():
            pair_copy(q).wait_send()
            half_copy(q).wait_send()

    for local in range(per_owner):
        q = me_t * per_owner + local
        whole_copy(q).wait_recv()
        for k in range(1, nx):
            src = lax.rem(me_x + k, nx)
            for c in range(2):
                ref = recv.at[src, pl.ds(c * half_rows, half_rows), pl.ds(local * W, W)]
                pltpu.make_async_remote_copy(
                    src_ref=ref, dst_ref=ref, send_sem=rs_s.at[0], recv_sem=rs_r.at[src, local, c], **device(sibling),
                ).wait_recv()


def finish_kernel(up_v, dn_v, recv, up_o, dn_o, mlp_o, total, sem):
    copies = [pltpu.make_async_copy(up_v, up_o, sem.at[0]), pltpu.make_async_copy(dn_v, dn_o, sem.at[1])]
    for c in copies:
        c.start()
    n, T, _ = recv.shape
    rows = 128

    @pl.loop(0, T // rows)
    def _(i):
        r = pl.ds(pl.multiple_of(i * rows, rows), rows)
        acc = recv[0, r, :].astype(jnp.float32)
        for k in range(1, n):
            acc += recv[k, r, :].astype(jnp.float32)
        total[r, :] = acc.astype(jnp.bfloat16)

    last = pltpu.make_async_copy(total, mlp_o, sem.at[2])
    last.start()
    for c in copies:
        c.wait()
    last.wait()


slot_kinds = "UUDUUDUUUDDDDD"
slot_pieces = (
    0xECA86420, 0xFDB97531,
    0xECA86420, 0xCA86420E,
    0xDB97531F, 0xFAB97531,
    0xA86420EC, 0xB97531FD,
    0x86420ECA, 0xAB97420E,
    0xB986531F, 0x987420EA,
    0x826531F0, 0xCD020EC0,
)
slot_live = (0xFF, 0xFF, 0xFF, 0xFF, 0xFF, 0xFF, 0xFF, 0xFF, 0xFF, 0xFF, 0xFF, 0xFF, 0xFE, 0xDE)
slot_tight = (0x00, 0x00, 0x00, 0x00, 0x00, 0x00, 0x00, 0x00, 0x00, 0x00, 0xC0, 0xC0, 0x80, 0x00)
relays = ((1, 12), (2, 13), (7, 11))
relay_place = 6
ring_places = 8
last_chunks = 4
second_leads = 0x0C
pairs_per_step = 2


def look(word, place, width):
    word = word - 2**32 if word >= 2**31 else word
    return lax.bitwise_and(lax.shift_right_logical(jnp.int32(word), place * width), jnp.int32(2**width - 1))


class Places:
    def __init__(self, n_fs, n_tp):
        nz, ny = grid_of(n_fs)
        self.n, self.nz, self.ny = n_fs, nz, ny
        self.me_f, self.me_t = lax.axis_index("fs"), lax.axis_index("tp")
        self.me_x, self.me_c = lax.div(self.me_t, 2), lax.rem(self.me_t, 2)
        z, y = lax.div(self.me_f, ny), lax.rem(self.me_f, ny)
        along = z + self.me_x * (nz - 1 - 2 * z)
        self.pos = along + y * (n_fs - 1 - 2 * along)
        self.seat = (self.pos, n_fs - 1 - self.pos)
        self.behind = tuple(lax.rem(p + n_fs - 1, n_fs) for p in self.seat)

    def at(self, p):
        side = lax.div(p, self.nz)
        along = p + side * (self.n - 1 - 2 * p)
        return (along + self.me_x * (self.nz - 1 - 2 * along)) * self.ny + side

    def mirrored(self, code, m):
        src, half = lax.div(code, 2), lax.rem(code, 2)
        return self.at(src + m * (self.n - 1 - 2 * src)), half + m * (1 - 2 * half)

    def piece(self, s, place, d):
        return self.mirrored(look(slot_pieces[s], place, 4), d)

    def live(self, s, place):
        return None if slot_live[s] == 2**self.n - 1 else look(slot_live[s], place, 1) == 1

    def last_tiles(self, per_owner):
        last = len(slot_kinds) - 1
        tiles = []
        for d in range(2):
            f, half = self.piece(last, self.behind[d], d)
            tiles.append(f * 2 + half)
        return self.live(last, self.behind[0]), tiles, lax.div(tiles[0], per_owner) == self.me_t


def routed_kernel(
    n_fs, n_tp, tokens, gain, up_l, dn_l, up_w, dn_w, recv, hid, x, part, stage, up_f, dn_f, gain_v, acc,
    loc_sem, tok_s, tok_r, ring_s, ring_r, y_s, y_r, pre_s, pre_r, rs_s, rs_r,
):
    here = Places(n_fs, n_tp)
    me_f, me_t, me_x, me_c, pos, at = here.me_f, here.me_t, here.me_x, here.me_c, here.pos, here.at
    seat, behind, mirrored, piece, live = here.seat, here.behind, here.mirrored, here.piece, here.live
    T, Dk = tokens.shape
    R, F = up_l.shape
    D = n_fs * R
    W = R // 2
    nx = n_tp // 2
    sibling = me_t + 1 - 2 * me_c
    half_rows = T // 2
    per_owner = Dk // W
    S = len(slot_kinds)
    last = S - 1

    right, left, across = at(lax.rem(pos + 1, n_fs)), at(lax.rem(pos + n_fs - 1, n_fs)), at(n_fs - 1 - pos)
    is_relay = (pos == relay_place) | (pos == n_fs - 1 - relay_place)

    def tp_peer(k):
        return lax.rem(me_t + k, n_tp)

    barrier = pltpu.get_barrier_semaphore()
    for f in (right, left, across):
        pl.semaphore_signal(barrier, inc=1, device_id={"fs": f, "tp": me_t}, device_id_type=MESH)
    for k in range(1, n_tp):
        pl.semaphore_signal(barrier, inc=1, device_id={"fs": me_f, "tp": tp_peer(k)}, device_id_type=MESH)

    def tok_cols(t):
        return x.at[:, pl.ds(pl.multiple_of(t * Dk, Dk), Dk)]

    quarter = W // 2
    gain_copy = pltpu.make_async_copy(gain, gain_v, loc_sem.at[0])
    firsts = [(h, c) for c in range(2) for h in range(2)]

    def up_copy(h, c):
        rows = pl.ds(h * W + c * quarter, quarter)
        return pltpu.make_async_copy(up_l.at[rows, :], up_f.at[rows, :], loc_sem.at[1 + 2 * h + c])

    tok_copy = pltpu.make_async_copy(tokens, tok_cols(me_t), loc_sem.at[5])
    dn_copy = pltpu.make_async_copy(dn_l, dn_f, loc_sem.at[6])
    gain_copy.start()
    for h, c in firsts:
        up_copy(h, c).start()

    def when(pred, body):
        if pred is None:
            body()
        else:
            pl.when(pred)(body)

    def chunks(s):
        return last_chunks if s == last else 2

    def index(s, c):
        return 2 * s + c

    def ref_of(kind, f, half, c, n):
        if kind == "U":
            rows = W // n
            return up_w.at[pl.ds(pl.multiple_of(f * R + half * W + c * rows, rows), rows), :]
        return dn_w.at[pl.ds(c * (F // n), F // n), pl.ds(pl.multiple_of(f * R + half * W, W), W)]

    def ring_copy(s, c, d, place):
        f, half = piece(s, place, d)
        ref = ref_of(slot_kinds[s], f, half, c, chunks(s))
        return pltpu.make_async_remote_copy(
            src_ref=ref, dst_ref=ref, send_sem=ring_s.at[d, index(s, c)], recv_sem=ring_r.at[d, index(s, c)],
            device_id={"fs": right if d == 0 else left, "tp": me_t}, device_id_type=MESH,
        )

    def send(s, c, sides=(0, 1), tight=None):
        for d in sides:
            pred = live(s, seat[d])
            if tight is not None:
                here_tight = (look(slot_tight[s], seat[d], 1) == 1) == tight
                pred = here_tight if pred is None else pred & here_tight
            when(pred, lambda: ring_copy(s, c, d, seat[d]).start())

    def arrive(s, c):
        for d in range(2):
            when(live(s, behind[d]), lambda: ring_copy(s, c, d, behind[d]).wait_recv())

    def relay_copy(j, m):
        f, half = mirrored(jnp.int32(relays[j][1]), m)
        ref = ref_of("D", f, half, 0, 1)
        return pltpu.make_async_remote_copy(
            src_ref=ref, dst_ref=ref, send_sem=y_s.at[j], recv_sem=y_r.at[j],
            device_id={"fs": across, "tp": me_t}, device_id_type=MESH,
        )

    relay_out = jnp.where(pos == relay_place, 0, 1)

    own_row = pl.multiple_of(me_f * R, R)
    early_core = jnp.where(me_c == me_x, 0, 1)
    leads = [look(second_leads, seat[d], 1) == early_core for d in range(2)]
    gain_copy.wait()
    spread = jnp.transpose(jnp.broadcast_to(gain_v[...], (128, R)))

    def convert(h, c):
        up_copy(h, c).wait()
        first = h * W + c * quarter
        for j in range(F // 128):
            cols = pl.ds(j * 128, 128)
            up_w[pl.ds(own_row + first, quarter), cols] = (
                spread[first : first + quarter] * up_f[pl.ds(first, quarter), cols]
            ).astype(jnp.bfloat16)

    for h, c in firsts:
        convert(h, c)
        if (h, c) == (0, 0):
            pl.semaphore_wait(barrier, n_tp + 2)
        pl.when(leads[h])(lambda: send(0, c, (h,)))
        if (h, c) == (1, 0):
            tok_copy.start()
            dn_copy.start()
    for d in range(2):
        @pl.when(leads[d])
        def _():
            for e in range(2):
                send(1, e, (d,))

    def token_copy(k):
        return pltpu.make_async_remote_copy(
            src_ref=tok_cols(me_t), dst_ref=tok_cols(me_t), send_sem=tok_s.at[k], recv_sem=tok_r.at[k],
            device_id={"fs": me_f, "tp": tp_peer(k)}, device_id_type=MESH,
        )

    tok_copy.wait()
    for k in range(1, n_tp):
        token_copy(k).start()
    dn_copy.wait()
    block = min(F, 256)

    @pl.loop(0, 2 * (F // block))
    def _(i):
        r = pl.ds(pl.multiple_of(lax.rem(i, F // block) * block, block), block)
        dn_w[r, pl.ds(own_row, R)] = jnp.transpose(dn_f[:, r]).astype(jnp.bfloat16)

    for d in range(2):
        @pl.when(jnp.logical_not(leads[d]))
        def _():
            for t in range(2):
                for e in range(2):
                    send(t, e, (d,))

    def normalise():
        for k in range(1, n_tp):
            src = lax.rem(me_t - k + n_tp, n_tp)
            pltpu.make_async_remote_copy(
                src_ref=tok_cols(src), dst_ref=tok_cols(src), send_sem=tok_s.at[k], recv_sem=tok_r.at[k],
                device_id={"fs": me_f, "tp": tp_peer(k)}, device_id_type=MESH,
            ).wait_recv()
            token_copy(k).wait_send()
        rows = 64

        @pl.loop(0, T // rows)
        def _(i):
            r = pl.ds(pl.multiple_of(i * rows, rows), rows)
            v = x[r, :].astype(jnp.float32)
            x[r, :] = (v * lax.rsqrt(jnp.mean(v * v, axis=-1, keepdims=True) + norm_floor)).astype(jnp.bfloat16)

    width = 256

    def make_hidden(first, count):
        @pl.loop(first, first + count)
        def _(i):
            c = pl.ds(pl.multiple_of(i * width, width), width)
            pre = jnp.dot(x[...], up_w[:, c], preferred_element_type=jnp.float32)
            hid[:, c] = jnp.square(jnp.maximum(pre, 0.0)).astype(jnp.bfloat16)

    my_half = pl.ds(pl.multiple_of(me_c * half_rows, half_rows), half_rows)
    its_half = pl.ds(pl.multiple_of((1 - me_c) * half_rows, half_rows), half_rows)

    def device(t):
        return dict(device_id={"fs": me_f, "tp": t}, device_id_type=MESH)

    def cols_of(q):
        return pl.ds(pl.multiple_of(lax.rem(q, per_owner) * W, W), W)

    def tile(q):
        return pl.ds(pl.multiple_of(q * W, W), W)

    def whole_copy(q):
        return pltpu.make_async_remote_copy(
            src_ref=part.at[q], dst_ref=recv.at[nx, :, cols_of(q)],
            send_sem=rs_s.at[q], recv_sem=rs_r.at[nx, lax.rem(q, per_owner), 0], **device(sibling),
        )

    def pair_copy(q):
        return pltpu.make_async_remote_copy(
            src_ref=part.at[q, its_half], dst_ref=stage.at[q],
            send_sem=pre_s.at[q], recv_sem=pre_r.at[q], **device(sibling),
        )

    def half_copy(q):
        return pltpu.make_async_remote_copy(
            src_ref=part.at[q, my_half], dst_ref=recv.at[me_x, my_half, cols_of(q)],
            send_sem=rs_s.at[q], recv_sem=rs_r.at[me_x, lax.rem(q, per_owner), me_c],
            **device(lax.div(q, per_owner)),
        )

    def pass_on(q):
        @pl.when(lax.div(q, 2 * per_owner) != me_x)
        def _():
            pair_copy(q).wait_recv()
            both = part[q, my_half, :].astype(jnp.float32) + stage[q].astype(jnp.float32)
            part[q, my_half, :] = both.astype(jnp.bfloat16)
            half_copy(q).start()

    def do_pair(q, ok):
        use = [jnp.where(ok[0] == 1, q[0], q[1]), jnp.where(ok[1] == 1, q[1], q[0])]

        @pl.loop(0, 2)
        def _(i):
            r = pl.ds(pl.multiple_of(lax.rem(i + 1 + me_c, 2) * half_rows, half_rows), half_rows)
            both = jnp.concatenate([dn_w[:, tile(u)] for u in use], axis=1)
            out = jnp.dot(hid[r, :], both, preferred_element_type=jnp.float32).astype(jnp.bfloat16)
            for j in range(2):
                owner = lax.div(q[j], per_owner)

                @pl.when(ok[j] == 1)
                def _():
                    part[q[j], r, :] = out[:, j * W : (j + 1) * W]

                    @pl.when((i == 0) & (lax.div(owner, nx) != me_x))
                    def _():
                        pair_copy(q[j]).start()

                    @pl.when((i == 1) & (owner == sibling))
                    def _():
                        whole_copy(q[j]).start()

    def entry_of(e):
        kind = e[0]
        if kind == "none":
            return jnp.int32(0), jnp.int32(0)
        if kind == "own":
            return me_f * 2 + e[1], jnp.int32(1)
        if kind == "relay":
            f, half = mirrored(jnp.int32(relays[e[1]][1]), 1 - relay_out)
            return f * 2 + half, jnp.where(is_relay, 1, 0)
        s, d = e[1], e[2]
        f, half = piece(s, behind[d], d)
        ok = jnp.int32(1) if slot_live[s] == 2**n_fs - 1 else look(slot_live[s], behind[d], 1)
        return f * 2 + half, ok

    def pick(i, values):
        out = values[0]
        for k in range(1, len(values)):
            out = jnp.where(i == k, values[k], out)
        return out

    def pass_pair(q, ok):
        for j in range(2):
            @pl.when(ok[j] == 1)
            def _():
                pass_on(q[j])

    def run_tiles(before, pairs):
        cur = [[entry_of(e) for e in pair] for pair in pairs]
        prev = [[entry_of(e) for e in before]] + cur[:-1]

        @pl.loop(0, len(pairs))
        def _(i):
            def chosen(table, j, what):
                return pick(i, [pair[j][what] for pair in table])

            q, ok = [[chosen(cur, j, what) for j in range(2)] for what in range(2)]

            @pl.when(ok[0] + ok[1] > 0)
            def _():
                do_pair(q, ok)

            pass_pair(*[[chosen(prev, j, what) for j in range(2)] for what in range(2)])

    tail_on, tail_q, tail_mine = here.last_tiles(per_owner)
    depth = F // last_chunks

    def across_copy(q, i):
        r = pl.ds(i * half_rows, half_rows)
        return pltpu.make_async_remote_copy(
            src_ref=part.at[q, r], dst_ref=recv.at[nx, r, cols_of(q)],
            send_sem=(rs_s, pre_s)[i].at[q], recv_sem=rs_r.at[nx, lax.rem(q, per_owner), i], **device(sibling),
        )

    def last_slot():
        for c in range(last_chunks):
            k = pl.ds(c * depth, depth)
            @pl.when(tail_on & jnp.logical_not(tail_mine))
            def _():
                for d in range(2):
                    ring_copy(last, c, d, behind[d]).wait_recv()
                for i in range(2):
                    r = pl.ds(i * half_rows, half_rows)
                    both = jnp.concatenate([dn_w[k, tile(q)] for q in tail_q], axis=1)
                    out = jnp.dot(hid[r, k], both, preferred_element_type=jnp.float32)
                    if c > 0:
                        out += acc[r, :]
                    if c < last_chunks - 1:
                        acc[r, :] = out
                    else:
                        for j, q in enumerate(tail_q):
                            part[q, r, :] = out[:, j * W : (j + 1) * W].astype(jnp.bfloat16)
                        for q in tail_q:
                            across_copy(q, i).start()

        settle()

        @pl.when(tail_on & tail_mine)
        def _():
            for c in range(last_chunks):
                for d in range(2):
                    ring_copy(last, c, d, behind[d]).wait_recv()

    def in_tail(q):
        return tail_on & ((q == tail_q[0]) | (q == tail_q[1]))

    def settle():
        @pl.loop(0, per_owner)
        def _(local):
            q = me_t * per_owner + local

            @pl.when(jnp.logical_not(in_tail(q)))
            def _():
                recv[me_x, :, cols_of(q)] = part[q]
                whole_copy(q).wait_recv()

            @pl.when(in_tail(q))
            def _():
                recv[me_x, :, cols_of(q)] = jnp.zeros((T, W), jnp.bfloat16)

        for local in range(per_owner):
            for k in range(1, nx):
                src = lax.rem(me_x + k, nx)
                for c in range(2):
                    ref = recv.at[src, pl.ds(c * half_rows, half_rows), pl.ds(local * W, W)]
                    pltpu.make_async_remote_copy(
                        src_ref=ref, dst_ref=ref, send_sem=rs_s.at[0], recv_sem=rs_r.at[src, local, c], **device(sibling),
                    ).wait_recv()

        @pl.loop(0, D // W)
        def _(q):
            owner = lax.div(q, per_owner)

            @pl.when((owner == sibling) & jnp.logical_not(in_tail(q)))
            def _():
                whole_copy(q).wait_send()

            @pl.when(lax.div(owner, nx) != me_x)
            def _():
                pair_copy(q).wait_send()
                half_copy(q).wait_send()

        for j in range(len(relays)):
            @pl.when(is_relay)
            def _():
                relay_copy(j, relay_out).wait_send()

    def wait_sends(slots):
        for s in slots:
            for c in range(chunks(s)):
                for d in range(2):
                    when(live(s, seat[d]), lambda: ring_copy(s, c, d, seat[d]).wait_send())

    def sends_after(s, c):
        if s + 1 < last and slot_tight[s + 1]:
            send(s + 1, c, tight=True)
        if s + 2 < last:
            send(s + 2, c, tight=False if slot_tight[s + 2] else None)
        if (s + 2, c) == (last, 1):
            for e in range(last_chunks):
                send(last, e)

    queue = [[("own", h) for h in range(2)]]
    hidden_from = 2 * max(s for s in range(S) if slot_kinds[s] == "U") + 1
    blocks = F // width
    per_step = (blocks + 1) // 2
    prior = [("none",)] * 2
    normal_at = max(0, hidden_from - 6)

    for s in range(S):
        for c in range(chunks(s)):
            k = index(s, c)
            if s == last:
                if c == 0:
                    wait_sends(range(last - 2))
                    last_slot()
                continue
            arrive(s, c)
            for j, (t, _) in enumerate(relays):
                if t + 1 == s and c == 0:
                    @pl.when(is_relay)
                    def _():
                        relay_copy(j, 1 - relay_out).wait_recv()
                    if j % 2 == 0:
                        queue.append([("relay", j), ("none",)])
                    elif queue and queue[-1][0] == ("relay", j - 1):
                        queue[-1][1] = ("relay", j)
                    else:
                        queue.append([("relay", j), ("none",)])
            sends_after(s, c)
            if c == 1 and s < last:
                for j, (t, _) in enumerate(relays):
                    if t == s + 1:
                        @pl.when(is_relay)
                        def _():
                            relay_copy(j, relay_out).start()
                if slot_kinds[s] == "D":
                    queue.append([("ring", s, d) for d in range(2)])
            if k == normal_at:
                normalise()
            if k in (hidden_from, hidden_from + 1):
                make_hidden((k - hidden_from) * per_step, min(per_step, blocks - (k - hidden_from) * per_step))
            if k > hidden_from + 1 and queue:
                count = len(queue) if (s, c) == (last - 1, 1) else pairs_per_step
                take, queue = queue[:count], queue[count:]
                run_tiles(prior, take)
                prior = take[-1]
                if not queue:
                    final = [entry_of(e) for e in prior]
                    pass_pair([e[0] for e in final], [e[1] for e in final])
                    prior = [("none",)] * 2

    wait_sends(range(last - 2, S))

    @pl.when(tail_on & jnp.logical_not(tail_mine))
    def _():
        for q in tail_q:
            for i in range(2):
                across_copy(q, i).wait_send()

    @pl.when(tail_on & tail_mine)
    def _():
        for q in tail_q:
            for i in range(2):
                across_copy(q, i).wait_recv()


def routed_finish(n_fs, n_tp, up_v, dn_v, recv, hid, up_o, dn_o, mlp_o, total, out, sem):
    here = Places(n_fs, n_tp)
    n, T, Dk = recv.shape
    W = up_v.shape[0] // n_fs // 2
    per_owner = Dk // W
    copies = []
    for k, (v, o) in enumerate(((up_v, up_o), (dn_v, dn_o))):
        half = v.shape[0] // 2
        copies += [
            pltpu.make_async_copy(v.at[pl.ds(h * half, half), :], o.at[pl.ds(h * half, half), :], sem.at[2 * k + h])
            for h in range(2)
        ]
    for c in copies:
        c.start()
    tail_on, tail_q, tail_mine = here.last_tiles(per_owner)
    rows = 128

    @pl.loop(0, T // rows)
    def _(i):
        r = pl.ds(pl.multiple_of(i * rows, rows), rows)
        acc = recv[0, r, :].astype(jnp.float32)
        for k in range(1, n):
            acc += recv[k, r, :].astype(jnp.float32)
        total[r, :] = acc

    @pl.when(tail_on & tail_mine)
    def _():
        @pl.loop(0, 2)
        def _(i):
            r = pl.ds(pl.multiple_of(i * (T // 2), T // 2), T // 2)
            both = jnp.concatenate([dn_v[:, pl.ds(pl.multiple_of(q * W, W), W)] for q in tail_q], axis=1)
            late = jnp.dot(hid[r, :], both, preferred_element_type=jnp.float32).astype(jnp.bfloat16)
            for j, q in enumerate(tail_q):
                cols = pl.ds(pl.multiple_of(lax.rem(q, per_owner) * W, W), W)
                total[r, cols] += late[:, j * W : (j + 1) * W].astype(jnp.float32)

    @pl.loop(0, T // rows)
    def _(i):
        r = pl.ds(pl.multiple_of(i * rows, rows), rows)
        out[r, :] = total[r, :].astype(jnp.bfloat16)

    written = pltpu.make_async_copy(out, mlp_o, sem.at[4])
    written.start()
    for c in copies:
        c.wait()
    written.wait()


def solution(mesh):
    n_fs, n_tp = mesh.shape["fs"], mesh.shape["tp"]
    bf16 = jnp.bfloat16

    def routed(tokens, norm_gain, up_master, down_master):
        T, Dk = tokens.shape
        R, F = up_master.shape
        D, W = n_fs * R, R // 2
        waves = 2 * len(slot_kinds) + last_chunks - 2
        hbm_spec = pl.BlockSpec(memory_space=pltpu.HBM)
        vmem_spec = pl.BlockSpec(memory_space=pltpu.VMEM)
        dma = pltpu.SemaphoreType.DMA
        held = pl.pallas_call(
            functools.partial(routed_kernel, n_fs, n_tp),
            out_shape=(
                pltpu.VMEM((D, F), bf16),
                pltpu.VMEM((F, D), bf16),
                pltpu.VMEM((n_tp // 2 + 1, T, Dk), bf16),
                pltpu.VMEM((T, F), bf16),
            ),
            in_specs=[hbm_spec] * 4,
            out_specs=(vmem_spec,) * 4,
            scratch_shapes=[
                pltpu.VMEM((T, D), bf16),
                pltpu.VMEM((D // W, T, W), bf16),
                pltpu.VMEM((D // W, T // 2, W), bf16),
                pltpu.VMEM((R, F), jnp.float32),
                pltpu.VMEM((R, F), jnp.float32),
                pltpu.VMEM((1, R), jnp.float32),
                pltpu.VMEM((T, 2 * W), jnp.float32),
                dma((7,)),
                dma((n_tp,)),
                dma((n_tp,)),
                dma((2, waves)),
                dma((2, waves)),
                dma((len(relays),)),
                dma((len(relays),)),
                dma((D // W,)),
                dma((D // W,)),
                dma((D // W,)),
                dma((n_tp // 2 + 1, Dk // W, 2)),
            ],
            compiler_params=pltpu.CompilerParams(
                collective_id=0, has_side_effects=True, vmem_limit_bytes=40 * 2**20
            ),
        )(tokens, norm_gain[None, :], up_master, down_master)
        return pl.pallas_call(
            functools.partial(routed_finish, n_fs, n_tp),
            out_shape=(
                jax.ShapeDtypeStruct((D, F), bf16),
                jax.ShapeDtypeStruct((F, D), bf16),
                jax.ShapeDtypeStruct((T, Dk), bf16),
            ),
            in_specs=[vmem_spec] * 4,
            out_specs=(pl.BlockSpec(memory_space=pl.ANY),) * 3,
            scratch_shapes=[pltpu.VMEM((T, Dk), jnp.float32), pltpu.VMEM((T, Dk), bf16), dma((5,))],
            compiler_params=pltpu.CompilerParams(vmem_limit_bytes=12 * 2**20),
        )(*held)

    def on_device(tokens, norm_gain, up_master, down_master):
        T, Dk = tokens.shape
        R, F = up_master.shape
        D = n_fs * R
        W = R // 2 if (R // 2) % 128 == 0 else R
        S = len(send_list(n_fs))
        any_spec = pl.BlockSpec(memory_space=pl.ANY)
        vmem_spec = pl.BlockSpec(memory_space=pltpu.VMEM)
        if (n_fs, grid_of(n_fs)[1], n_tp * grid_of(n_fs)[1], 2 * W) == (ring_places, 2, n_fs, R):
            return routed(tokens, norm_gain, up_master, down_master)
        up_v, dn_v, recv = pl.pallas_call(
            functools.partial(gather_kernel, n_fs, n_tp),
            out_shape=(pltpu.VMEM((D, F), bf16), pltpu.VMEM((F, D), bf16), pltpu.VMEM((n_tp // 2 + 1, T, Dk), bf16)),
            in_specs=[pl.BlockSpec(memory_space=pltpu.HBM)] * 4,
            out_specs=(vmem_spec,) * 3,
            scratch_shapes=[
                pltpu.VMEM((T, D), bf16),
                pltpu.VMEM((T, F), bf16),
                pltpu.VMEM((D // W, T, W), bf16),
                pltpu.VMEM((D // W, T // 2, W), bf16),
                pltpu.VMEM((R, F), jnp.float32),
                pltpu.VMEM((R, F), jnp.float32),
                pltpu.VMEM((1, R), jnp.float32),
                pltpu.SemaphoreType.DMA((4,)),
                pltpu.SemaphoreType.DMA((n_tp,)),
                pltpu.SemaphoreType.DMA((n_tp,)),
                pltpu.SemaphoreType.DMA((2, S)),
                pltpu.SemaphoreType.DMA((2, S)),
                pltpu.SemaphoreType.DMA((D // W,)),
                pltpu.SemaphoreType.DMA((D // W,)),
                pltpu.SemaphoreType.DMA((D // W,)),
                pltpu.SemaphoreType.DMA((n_tp // 2 + 1, Dk // W, 2)),
            ],
            compiler_params=pltpu.CompilerParams(
                collective_id=0, has_side_effects=True, vmem_limit_bytes=44 * 2**20
            ),
        )(tokens, norm_gain[None, :], up_master, down_master)
        return pl.pallas_call(
            finish_kernel,
            out_shape=(
                jax.ShapeDtypeStruct((D, F), bf16),
                jax.ShapeDtypeStruct((F, D), bf16),
                jax.ShapeDtypeStruct((T, Dk), bf16),
            ),
            in_specs=[vmem_spec] * 3,
            out_specs=(any_spec,) * 3,
            scratch_shapes=[pltpu.VMEM((T, Dk), bf16), pltpu.SemaphoreType.DMA((3,))],
            compiler_params=pltpu.CompilerParams(vmem_limit_bytes=8 * 2**20),
        )(up_v, dn_v, recv)

    in_specs = (P("fs", "tp"), P("fs"), P("fs", "tp"), P("fs", "tp"))
    out_specs = (P(None, "tp"), P("tp", None), P("fs", "tp"))
    return jax.shard_map(on_device, mesh=mesh, in_specs=in_specs, out_specs=out_specs, check_vma=False)
```

```python
import functools

import jax
import jax.numpy as jnp
from jax import lax
from jax.experimental import pallas as pl
from jax.experimental.pallas import tpu as pltpu
from jax.sharding import PartitionSpec as P

norm_floor = 1e-06
MESH = pl.DeviceIdType.MESH


def grid_of(n):
    ny = max(d for d in range(1, n + 1) if n % d == 0 and d * d <= n)
    return n // ny, ny


def position_of(f, nz, ny):
    if ny == 1:
        return f
    z, y = lax.div(f, ny), lax.rem(f, ny)
    tail = lax.div(y + (ny - 1), ny)
    k = nz - 1 - z
    odd = lax.rem(k, 2)
    r = (1 - odd) * (y - 1) + odd * (ny - 1 - y)
    return (1 - tail) * z + tail * (nz + k * (ny - 1) + r)


def index_at(p, nz, ny):
    if ny == 1:
        return p
    tail = lax.div(lax.div(p, nz) + (ny - 2), ny - 1)
    q = tail * (p - nz)
    k = lax.div(q, ny - 1)
    r = lax.rem(q, ny - 1)
    odd = lax.rem(k, 2)
    z = (1 - tail) * p + tail * (nz - 1 - k)
    y = tail * ((1 - odd) * (1 + r) + odd * (ny - 1 - r))
    return z * ny + y


def send_list(n):
    hops = n // 2
    split = n % 2 == 0

    def pieces(a, h):
        return [(a, h, 0)] if split and h == hops - 1 else [(a, h, 0), (a, h, 1)]

    ups = [p for h in range(1, hops) for p in pieces("u", h)]
    downs = [p for h in range(1, hops) for p in pieces("d", h)]
    own_u, own_d = pieces("u", 0), pieces("d", 0)
    return own_u + own_d[:1] + ups + own_d[1:] + downs


def gather_kernel(
    n_fs, n_tp, tokens, gain, up_l, dn_l, up_w, dn_w, recv, x, hid, part, stage, up_f, dn_f, gain_v,
    loc_sem, tok_s, tok_r, ring_s, ring_r, pre_s, pre_r, rs_s, rs_r,
):
    nz, ny = grid_of(n_fs)
    me_f, me_t = lax.axis_index("fs"), lax.axis_index("tp")
    pos = position_of(me_f, nz, ny)
    T, Dk = tokens.shape
    R, F = up_l.shape
    D = n_fs * R
    split_cols = (R // 2) % 128 == 0
    W = R // 2 if split_cols else R

    def at(offset):
        return index_at(lax.rem(pos + offset + n_fs, n_fs), nz, ny)

    right, left = at(1), at(-1)

    def tp_peer(k):
        return lax.rem(me_t + k, n_tp)

    barrier = pltpu.get_barrier_semaphore()
    for f in (right, left):
        pl.semaphore_signal(barrier, inc=1, device_id={"fs": f, "tp": me_t}, device_id_type=MESH)
    for k in range(1, n_tp):
        pl.semaphore_signal(barrier, inc=1, device_id={"fs": me_f, "tp": tp_peer(k)}, device_id_type=MESH)

    def up_piece(f, h):
        return up_w.at[pl.ds(pl.multiple_of(f * R + h * (R // 2), R // 2), R // 2), :]

    def dn_piece(f, h):
        if split_cols:
            return dn_w.at[:, pl.ds(pl.multiple_of(f * R + h * (R // 2), R // 2), R // 2)]
        return dn_w.at[pl.ds(h * (F // 2), F // 2), pl.ds(pl.multiple_of(f * R, R), R)]

    def tok_cols(t):
        return x.at[:, pl.ds(pl.multiple_of(t * Dk, Dk), Dk)]

    own = [
        pltpu.make_async_copy(up_l, up_f, loc_sem.at[0]),
        pltpu.make_async_copy(tokens, tok_cols(me_t), loc_sem.at[1]),
        pltpu.make_async_copy(dn_l, dn_f, loc_sem.at[2]),
    ]
    gain_copy = pltpu.make_async_copy(gain, gain_v, loc_sem.at[3])
    for c in [gain_copy] + own:
        c.start()
    own_rows = pl.ds(pl.multiple_of(me_f * R, R), R)
    gain_copy.wait()
    spread = jnp.transpose(jnp.broadcast_to(gain_v[...], (128, R)))
    own[0].wait()
    for c in range(F // 128):
        cols = pl.ds(c * 128, 128)
        up_w[own_rows, cols] = (spread * up_f[:, cols]).astype(jnp.bfloat16)
    own[1].wait()
    pl.semaphore_wait(barrier, n_tp + 1)

    order = send_list(n_fs)
    S = len(order)

    def ring_copy(s, d):
        a, hop, second = order[s]
        half = second if d == 0 else 1 - second
        f = at(-hop if d == 0 else hop)
        ref = up_piece(f, half) if a == "u" else dn_piece(f, half)
        return pltpu.make_async_remote_copy(
            src_ref=ref, dst_ref=ref, send_sem=ring_s.at[d, s], recv_sem=ring_r.at[d, s],
            device_id={"fs": right if d == 0 else left, "tp": me_t}, device_id_type=MESH,
        )

    def arrival(s, d):
        a, hop, second = order[s]
        half = second if d == 0 else 1 - second
        f = at(-(hop + 1) if d == 0 else hop + 1)
        return f, half, (up_piece(f, half) if a == "u" else dn_piece(f, half))

    def wait_arrival(s, d):
        f, half, ref = arrival(s, d)
        pltpu.make_async_remote_copy(
            src_ref=ref, dst_ref=ref, send_sem=ring_s.at[d, s], recv_sem=ring_r.at[d, s],
            device_id={"fs": right if d == 0 else left, "tp": me_t}, device_id_type=MESH,
        ).wait_recv()

    needs = [-1 if hop == 0 else order.index((a, hop - 1, second)) for a, hop, second in order]
    issued = [0]

    def issue(upto):
        while issued[0] < S and needs[issued[0]] <= upto:
            if upto < 0 and issued[0] >= 3:
                break
            for d in range(2):
                ring_copy(issued[0], d).start()
            issued[0] += 1

    for s in range(2):
        for d in range(2):
            ring_copy(s, d).start()

    def token_copy(k):
        return pltpu.make_async_remote_copy(
            src_ref=tok_cols(me_t), dst_ref=tok_cols(me_t), send_sem=tok_s.at[k], recv_sem=tok_r.at[k],
            device_id={"fs": me_f, "tp": tp_peer(k)}, device_id_type=MESH,
        )

    for k in range(1, n_tp):
        token_copy(k).start()
    own[2].wait()
    block = min(F, 256)

    @pl.loop(0, F // block)
    def _(i):
        r = pl.ds(pl.multiple_of(i * block, block), block)
        dn_w[r, own_rows] = jnp.transpose(dn_f[:, r]).astype(jnp.bfloat16)

    issued[0] = 2
    issue(-1)

    def normalise():
        for k in range(1, n_tp):
            src = lax.rem(me_t - k + n_tp, n_tp)
            pltpu.make_async_remote_copy(
                src_ref=tok_cols(src), dst_ref=tok_cols(src), send_sem=tok_s.at[k], recv_sem=tok_r.at[k],
                device_id={"fs": me_f, "tp": tp_peer(k)}, device_id_type=MESH,
            ).wait_recv()
            token_copy(k).wait_send()
        rows = 64

        @pl.loop(0, T // rows)
        def _(i):
            r = pl.ds(pl.multiple_of(i * rows, rows), rows)
            v = x[r, :].astype(jnp.float32)
            x[r, :] = (v * lax.rsqrt(jnp.mean(v * v, axis=-1, keepdims=True) + norm_floor)).astype(jnp.bfloat16)

    def make_hidden():
        width = 256

        @pl.loop(0, F // width)
        def _(i):
            c = pl.ds(pl.multiple_of(i * width, width), width)
            pre = jnp.dot(x[...], up_w[:, c], preferred_element_type=jnp.float32)
            hid[:, c] = jnp.square(jnp.maximum(pre, 0.0)).astype(jnp.bfloat16)

    per_owner = Dk // W
    nx = n_tp // 2
    half_rows = T // 2
    me_x, me_c = lax.div(me_t, 2), lax.rem(me_t, 2)
    sibling = me_t + 1 - 2 * me_c
    my_half = pl.ds(pl.multiple_of(me_c * half_rows, half_rows), half_rows)
    its_half = pl.ds(pl.multiple_of((1 - me_c) * half_rows, half_rows), half_rows)

    def device(t):
        return dict(device_id={"fs": me_f, "tp": t}, device_id_type=MESH)

    def cols_of(q):
        return pl.ds(pl.multiple_of(lax.rem(q, per_owner) * W, W), W)

    def whole_copy(q):
        return pltpu.make_async_remote_copy(
            src_ref=part.at[q], dst_ref=recv.at[nx, :, cols_of(q)],
            send_sem=rs_s.at[q], recv_sem=rs_r.at[nx, lax.rem(q, per_owner), 0], **device(sibling),
        )

    def pair_copy(q):
        return pltpu.make_async_remote_copy(
            src_ref=part.at[q, its_half], dst_ref=stage.at[q],
            send_sem=pre_s.at[q], recv_sem=pre_r.at[q], **device(sibling),
        )

    def half_copy(q):
        return pltpu.make_async_remote_copy(
            src_ref=part.at[q, my_half], dst_ref=recv.at[me_x, my_half, cols_of(q)],
            send_sem=rs_s.at[q], recv_sem=rs_r.at[me_x, lax.rem(q, per_owner), me_c],
            **device(lax.div(q, per_owner)),
        )

    def pass_on(q):
        @pl.when(lax.div(q, 2 * per_owner) != me_x)
        def _():
            pair_copy(q).wait_recv()
            both = part[q, my_half, :].astype(jnp.float32) + stage[q].astype(jnp.float32)
            part[q, my_half, :] = both.astype(jnp.bfloat16)
            half_copy(q).start()

    def do_parts(first, count):
        c = pl.ds(pl.multiple_of(first * W, W), count * W)

        @pl.loop(0, 2)
        def _(i):
            r = pl.ds(pl.multiple_of(lax.rem(i + 1 + me_c, 2) * half_rows, half_rows), half_rows)
            out = jnp.dot(hid[r, :], dn_w[:, c], preferred_element_type=jnp.float32).astype(jnp.bfloat16)
            for k in range(count):
                part[first + k, r, :] = out[:, k * W : (k + 1) * W]
            for k in range(count):
                owner = lax.div(first + k, per_owner)

                @pl.when((i == 0) & (lax.div(owner, 2) != me_x))
                def _():
                    pair_copy(first + k).start()

                @pl.when((i == 1) & (owner == sibling))
                def _():
                    whole_copy(first + k).start()

    per_chunk = R // W
    ready = [(me_f * per_chunk, per_chunk)]
    last_up = max(s for s in range(S) if order[s][0] == "u")
    norm_at = max(0, last_up - 2)
    for s in range(S):
        for d in range(2):
            wait_arrival(s, d)
        issue(s)
        a, hop, _ = order[s]
        if a == "d" and split_cols:
            if n_fs % 2 == 0 and hop == n_fs // 2 - 1:
                ready.append((at(hop + 1) * 2, 2))
            else:
                for d in range(2):
                    f, half, _ = arrival(s, d)
                    ready.append((f * 2 + half, 1))
        if s == norm_at:
            normalise()
        if s == last_up:
            make_hidden()
        if s >= last_up:
            for first, count in ready:
                do_parts(first, count)
            for first, count in ready:
                for k in range(count):
                    pass_on(first + k)
            ready = []
    if not split_cols:
        @pl.loop(0, n_fs)
        def _(q):
            @pl.when(q != me_f)
            def _():
                do_parts(q, 1)
                pass_on(q)

    @pl.loop(0, per_owner)
    def _(local):
        cols = pl.ds(pl.multiple_of(local * W, W), W)
        recv[me_x, :, cols] = part[me_t * per_owner + local]

    for d in range(2):
        for s in range(S):
            ring_copy(s, d).wait_send()

    @pl.loop(0, D // W)
    def _(q):
        owner = lax.div(q, per_owner)

        @pl.when(owner == sibling)
        def _():
            whole_copy(q).wait_send()

        @pl.when(lax.div(owner, 2) != me_x)
        def _():
            pair_copy(q).wait_send()
            half_copy(q).wait_send()

    for local in range(per_owner):
        q = me_t * per_owner + local
        whole_copy(q).wait_recv()
        for k in range(1, nx):
            src = lax.rem(me_x + k, nx)
            for c in range(2):
                ref = recv.at[src, pl.ds(c * half_rows, half_rows), pl.ds(local * W, W)]
                pltpu.make_async_remote_copy(
                    src_ref=ref, dst_ref=ref, send_sem=rs_s.at[0], recv_sem=rs_r.at[src, local, c], **device(sibling),
                ).wait_recv()


def finish_kernel(up_v, dn_v, recv, up_o, dn_o, mlp_o, total, sem):
    copies = [pltpu.make_async_copy(up_v, up_o, sem.at[0]), pltpu.make_async_copy(dn_v, dn_o, sem.at[1])]
    for c in copies:
        c.start()
    n, T, _ = recv.shape
    rows = 128

    @pl.loop(0, T // rows)
    def _(i):
        r = pl.ds(pl.multiple_of(i * rows, rows), rows)
        acc = recv[0, r, :].astype(jnp.float32)
        for k in range(1, n):
            acc += recv[k, r, :].astype(jnp.float32)
        total[r, :] = acc.astype(jnp.bfloat16)

    last = pltpu.make_async_copy(total, mlp_o, sem.at[2])
    last.start()
    for c in copies:
        c.wait()
    last.wait()


slot_kinds = "UUDUUDUUUDDDDD"
slot_pieces = (
    0xECA86420, 0xFDB97531,
    0xECA86420, 0xCA86420E,
    0xDB97531F, 0xFAB97531,
    0xA86420EC, 0xB97531FD,
    0x86420ECA, 0xAB97420E,
    0xB986531F, 0x987420EA,
    0x826531F0, 0xCD020EC0,
)
slot_live = (0xFF, 0xFF, 0xFF, 0xFF, 0xFF, 0xFF, 0xFF, 0xFF, 0xFF, 0xFF, 0xFF, 0xFF, 0xFE, 0xDE)
slot_tight = (0x00, 0x00, 0x00, 0x00, 0x00, 0x00, 0x00, 0x00, 0x00, 0x00, 0xC0, 0xC0, 0x80, 0x00)
relays = ((1, 12), (2, 13), (7, 11))
relay_place = 6
ring_places = 8
last_chunks = 4
second_leads = 0x0C
pairs_per_step = 2


def look(word, place, width):
    word = word - 2**32 if word >= 2**31 else word
    return lax.bitwise_and(lax.shift_right_logical(jnp.int32(word), place * width), jnp.int32(2**width - 1))


class Places:
    def __init__(self, n_fs, n_tp):
        nz, ny = grid_of(n_fs)
        self.n, self.nz, self.ny = n_fs, nz, ny
        self.me_f, self.me_t = lax.axis_index("fs"), lax.axis_index("tp")
        self.me_x, self.me_c = lax.div(self.me_t, 2), lax.rem(self.me_t, 2)
        z, y = lax.div(self.me_f, ny), lax.rem(self.me_f, ny)
        along = z + self.me_x * (nz - 1 - 2 * z)
        self.pos = along + y * (n_fs - 1 - 2 * along)
        self.seat = (self.pos, n_fs - 1 - self.pos)
        self.behind = tuple(lax.rem(p + n_fs - 1, n_fs) for p in self.seat)

    def at(self, p):
        side = lax.div(p, self.nz)
        along = p + side * (self.n - 1 - 2 * p)
        return (along + self.me_x * (self.nz - 1 - 2 * along)) * self.ny + side

    def mirrored(self, code, m):
        src, half = lax.div(code, 2), lax.rem(code, 2)
        return self.at(src + m * (self.n - 1 - 2 * src)), half + m * (1 - 2 * half)

    def piece(self, s, place, d):
        return self.mirrored(look(slot_pieces[s], place, 4), d)

    def live(self, s, place):
        return None if slot_live[s] == 2**self.n - 1 else look(slot_live[s], place, 1) == 1

    def last_tiles(self, per_owner):
        last = len(slot_kinds) - 1
        tiles = []
        for d in range(2):
            f, half = self.piece(last, self.behind[d], d)
            tiles.append(f * 2 + half)
        return self.live(last, self.behind[0]), tiles, lax.div(tiles[0], per_owner) == self.me_t


def routed_kernel(
    n_fs, n_tp, tokens, gain, up_l, dn_l, up_w, dn_w, recv, hid, x, part, stage, up_f, dn_f, gain_v, acc,
    loc_sem, tok_s, tok_r, ring_s, ring_r, y_s, y_r, pre_s, pre_r, rs_s, rs_r,
):
    R, F = up_l.shape
    W = R // 2
    quarter = W // 2
    gain_copy = pltpu.make_async_copy(gain, gain_v, loc_sem.at[0])
    firsts = [(h, c) for c in range(2) for h in range(2)]

    def up_copy(h, c):
        rows = pl.ds(h * W + c * quarter, quarter)
        return pltpu.make_async_copy(up_l.at[rows, :], up_f.at[rows, :], loc_sem.at[1 + 2 * h + c])

    gain_copy.start()
    for h, c in firsts:
        up_copy(h, c).start()

    here = Places(n_fs, n_tp)
    me_f, me_t, me_x, me_c, pos, at = here.me_f, here.me_t, here.me_x, here.me_c, here.pos, here.at
    seat, behind, mirrored, piece, live = here.seat, here.behind, here.mirrored, here.piece, here.live
    T, Dk = tokens.shape
    R, F = up_l.shape
    D = n_fs * R
    W = R // 2
    nx = n_tp // 2
    sibling = me_t + 1 - 2 * me_c
    half_rows = T // 2
    per_owner = Dk // W
    S = len(slot_kinds)
    last = S - 1

    right, left, across = at(lax.rem(pos + 1, n_fs)), at(lax.rem(pos + n_fs - 1, n_fs)), at(n_fs - 1 - pos)
    is_relay = (pos == relay_place) | (pos == n_fs - 1 - relay_place)

    def tp_peer(k):
        return lax.rem(me_t + k, n_tp)

    barrier = pltpu.get_barrier_semaphore()
    for f in (right, left, across):
        pl.semaphore_signal(barrier, inc=1, device_id={"fs": f, "tp": me_t}, device_id_type=MESH)
    for k in range(1, n_tp):
        pl.semaphore_signal(barrier, inc=1, device_id={"fs": me_f, "tp": tp_peer(k)}, device_id_type=MESH)

    def tok_cols(t):
        return x.at[:, pl.ds(pl.multiple_of(t * Dk, Dk), Dk)]

    tok_copy = pltpu.make_async_copy(tokens, tok_cols(me_t), loc_sem.at[5])
    dn_copy = pltpu.make_async_copy(dn_l, dn_f, loc_sem.at[6])

    def when(pred, body):
        if pred is None:
            body()
        else:
            pl.when(pred)(body)

    def chunks(s):
        return last_chunks if s == last else 2

    def index(s, c):
        return 2 * s + c

    def ref_of(kind, f, half, c, n):
        if kind == "U":
            rows = W // n
            return up_w.at[pl.ds(pl.multiple_of(f * R + half * W + c * rows, rows), rows), :]
        return dn_w.at[pl.ds(c * (F // n), F // n), pl.ds(pl.multiple_of(f * R + half * W, W), W)]

    def ring_copy(s, c, d, place):
        f, half = piece(s, place, d)
        ref = ref_of(slot_kinds[s], f, half, c, chunks(s))
        return pltpu.make_async_remote_copy(
            src_ref=ref, dst_ref=ref, send_sem=ring_s.at[d, index(s, c)], recv_sem=ring_r.at[d, index(s, c)],
            device_id={"fs": right if d == 0 else left, "tp": me_t}, device_id_type=MESH,
        )

    def send(s, c, sides=(0, 1), tight=None):
        for d in sides:
            pred = live(s, seat[d])
            if tight is not None:
                here_tight = (look(slot_tight[s], seat[d], 1) == 1) == tight
                pred = here_tight if pred is None else pred & here_tight
            when(pred, lambda: ring_copy(s, c, d, seat[d]).start())

    def arrive(s, c):
        for d in range(2):
            when(live(s, behind[d]), lambda: ring_copy(s, c, d, behind[d]).wait_recv())

    def relay_copy(j, m):
        f, half = mirrored(jnp.int32(relays[j][1]), m)
        ref = ref_of("D", f, half, 0, 1)
        return pltpu.make_async_remote_copy(
            src_ref=ref, dst_ref=ref, send_sem=y_s.at[j], recv_sem=y_r.at[j],
            device_id={"fs": across, "tp": me_t}, device_id_type=MESH,
        )

    relay_out = jnp.where(pos == relay_place, 0, 1)

    own_row = pl.multiple_of(me_f * R, R)
    early_core = jnp.where(me_c == me_x, 0, 1)
    leads = [look(second_leads, seat[d], 1) == early_core for d in range(2)]
    gain_copy.wait()
    spread = jnp.transpose(jnp.broadcast_to(gain_v[...], (128, R)))

    def convert(h, c):
        up_copy(h, c).wait()
        first = h * W + c * quarter
        for j in range(F // 128):
            cols = pl.ds(j * 128, 128)
            up_w[pl.ds(own_row + first, quarter), cols] = (
                spread[first : first + quarter] * up_f[pl.ds(first, quarter), cols]
            ).astype(jnp.bfloat16)

    for h, c in firsts:
        convert(h, c)
        if (h, c) == (0, 0):
            pl.semaphore_wait(barrier, n_tp + 2)
        pl.when(leads[h])(lambda: send(0, c, (h,)))
        if (h, c) == (1, 0):
            tok_copy.start()
            dn_copy.start()
    for d in range(2):
        @pl.when(leads[d])
        def _():
            for e in range(2):
                send(1, e, (d,))

    def token_copy(k):
        return pltpu.make_async_remote_copy(
            src_ref=tok_cols(me_t), dst_ref=tok_cols(me_t), send_sem=tok_s.at[k], recv_sem=tok_r.at[k],
            device_id={"fs": me_f, "tp": tp_peer(k)}, device_id_type=MESH,
        )

    tok_copy.wait()
    for k in range(1, n_tp):
        token_copy(k).start()
    dn_copy.wait()
    block = min(F, 256)

    @pl.loop(0, 2 * (F // block))
    def _(i):
        r = pl.ds(pl.multiple_of(lax.rem(i, F // block) * block, block), block)
        dn_w[r, pl.ds(own_row, R)] = jnp.transpose(dn_f[:, r]).astype(jnp.bfloat16)

    for d in range(2):
        @pl.when(jnp.logical_not(leads[d]))
        def _():
            for t in range(2):
                for e in range(2):
                    send(t, e, (d,))

    def normalise():
        for k in range(1, n_tp):
            src = lax.rem(me_t - k + n_tp, n_tp)
            pltpu.make_async_remote_copy(
                src_ref=tok_cols(src), dst_ref=tok_cols(src), send_sem=tok_s.at[k], recv_sem=tok_r.at[k],
                device_id={"fs": me_f, "tp": tp_peer(k)}, device_id_type=MESH,
            ).wait_recv()
            token_copy(k).wait_send()
        rows = 64

        @pl.loop(0, T // rows)
        def _(i):
            r = pl.ds(pl.multiple_of(i * rows, rows), rows)
            v = x[r, :].astype(jnp.float32)
            x[r, :] = (v * lax.rsqrt(jnp.mean(v * v, axis=-1, keepdims=True) + norm_floor)).astype(jnp.bfloat16)

    width = 256

    def make_hidden(first, count):
        @pl.loop(first, first + count)
        def _(i):
            c = pl.ds(pl.multiple_of(i * width, width), width)
            pre = jnp.dot(x[...], up_w[:, c], preferred_element_type=jnp.float32)
            hid[:, c] = jnp.square(jnp.maximum(pre, 0.0)).astype(jnp.bfloat16)

    my_half = pl.ds(pl.multiple_of(me_c * half_rows, half_rows), half_rows)
    its_half = pl.ds(pl.multiple_of((1 - me_c) * half_rows, half_rows), half_rows)

    def device(t):
        return dict(device_id={"fs": me_f, "tp": t}, device_id_type=MESH)

    def cols_of(q):
        return pl.ds(pl.multiple_of(lax.rem(q, per_owner) * W, W), W)

    def tile(q):
        return pl.ds(pl.multiple_of(q * W, W), W)

    def whole_copy(q):
        return pltpu.make_async_remote_copy(
            src_ref=part.at[q], dst_ref=recv.at[nx, :, cols_of(q)],
            send_sem=rs_s.at[q], recv_sem=rs_r.at[nx, lax.rem(q, per_owner), 0], **device(sibling),
        )

    def pair_copy(q):
        return pltpu.make_async_remote_copy(
            src_ref=part.at[q, its_half], dst_ref=stage.at[q],
            send_sem=pre_s.at[q], recv_sem=pre_r.at[q], **device(sibling),
        )

    def half_copy(q):
        return pltpu.make_async_remote_copy(
            src_ref=part.at[q, my_half], dst_ref=recv.at[me_x, my_half, cols_of(q)],
            send_sem=rs_s.at[q], recv_sem=rs_r.at[me_x, lax.rem(q, per_owner), me_c],
            **device(lax.div(q, per_owner)),
        )

    def pass_on(q):
        @pl.when(lax.div(q, 2 * per_owner) != me_x)
        def _():
            pair_copy(q).wait_recv()
            both = part[q, my_half, :].astype(jnp.float32) + stage[q].astype(jnp.float32)
            part[q, my_half, :] = both.astype(jnp.bfloat16)
            half_copy(q).start()

    def do_pair(q, ok):
        use = [jnp.where(ok[0] == 1, q[0], q[1]), jnp.where(ok[1] == 1, q[1], q[0])]

        @pl.loop(0, 2)
        def _(i):
            r = pl.ds(pl.multiple_of(lax.rem(i + 1 + me_c, 2) * half_rows, half_rows), half_rows)
            both = jnp.concatenate([dn_w[:, tile(u)] for u in use], axis=1)
            out = jnp.dot(hid[r, :], both, preferred_element_type=jnp.float32).astype(jnp.bfloat16)
            for j in range(2):
                owner = lax.div(q[j], per_owner)

                @pl.when(ok[j] == 1)
                def _():
                    part[q[j], r, :] = out[:, j * W : (j + 1) * W]

                    @pl.when((i == 0) & (lax.div(owner, nx) != me_x))
                    def _():
                        pair_copy(q[j]).start()

                    @pl.when((i == 1) & (owner == sibling))
                    def _():
                        whole_copy(q[j]).start()

    def entry_of(e):
        kind = e[0]
        if kind == "none":
            return jnp.int32(0), jnp.int32(0)
        if kind == "own":
            return me_f * 2 + e[1], jnp.int32(1)
        if kind == "relay":
            f, half = mirrored(jnp.int32(relays[e[1]][1]), 1 - relay_out)
            return f * 2 + half, jnp.where(is_relay, 1, 0)
        s, d = e[1], e[2]
        f, half = piece(s, behind[d], d)
        ok = jnp.int32(1) if slot_live[s] == 2**n_fs - 1 else look(slot_live[s], behind[d], 1)
        return f * 2 + half, ok

    def pick(i, values):
        out = values[0]
        for k in range(1, len(values)):
            out = jnp.where(i == k, values[k], out)
        return out

    def pass_pair(q, ok):
        for j in range(2):
            @pl.when(ok[j] == 1)
            def _():
                pass_on(q[j])

    def run_tiles(before, pairs):
        cur = [[entry_of(e) for e in pair] for pair in pairs]
        prev = [[entry_of(e) for e in before]] + cur[:-1]

        @pl.loop(0, len(pairs))
        def _(i):
            def chosen(table, j, what):
                return pick(i, [pair[j][what] for pair in table])

            q, ok = [[chosen(cur, j, what) for j in range(2)] for what in range(2)]

            @pl.when(ok[0] + ok[1] > 0)
            def _():
                do_pair(q, ok)

            pass_pair(*[[chosen(prev, j, what) for j in range(2)] for what in range(2)])

    tail_on, tail_q, tail_mine = here.last_tiles(per_owner)
    depth = F // last_chunks

    def across_copy(q, i):
        r = pl.ds(i * half_rows, half_rows)
        return pltpu.make_async_remote_copy(
            src_ref=part.at[q, r], dst_ref=recv.at[nx, r, cols_of(q)],
            send_sem=(rs_s, pre_s)[i].at[q], recv_sem=rs_r.at[nx, lax.rem(q, per_owner), i], **device(sibling),
        )

    def last_slot():
        for c in range(last_chunks):
            k = pl.ds(c * depth, depth)
            @pl.when(tail_on & jnp.logical_not(tail_mine))
            def _():
                for d in range(2):
                    ring_copy(last, c, d, behind[d]).wait_recv()
                for i in range(2):
                    r = pl.ds(i * half_rows, half_rows)
                    both = jnp.concatenate([dn_w[k, tile(q)] for q in tail_q], axis=1)
                    out = jnp.dot(hid[r, k], both, preferred_element_type=jnp.float32)
                    if c > 0:
                        out += acc[r, :]
                    if c < last_chunks - 1:
                        acc[r, :] = out
                    else:
                        for j, q in enumerate(tail_q):
                            part[q, r, :] = out[:, j * W : (j + 1) * W].astype(jnp.bfloat16)
                        for q in tail_q:
                            across_copy(q, i).start()

        settle()

        @pl.when(tail_on & tail_mine)
        def _():
            for c in range(last_chunks):
                for d in range(2):
                    ring_copy(last, c, d, behind[d]).wait_recv()

    def in_tail(q):
        return tail_on & ((q == tail_q[0]) | (q == tail_q[1]))

    def settle():
        @pl.loop(0, per_owner)
        def _(local):
            q = me_t * per_owner + local

            @pl.when(jnp.logical_not(in_tail(q)))
            def _():
                recv[me_x, :, cols_of(q)] = part[q]
                whole_copy(q).wait_recv()

            @pl.when(in_tail(q))
            def _():
                recv[me_x, :, cols_of(q)] = jnp.zeros((T, W), jnp.bfloat16)

        for local in range(per_owner):
            for k in range(1, nx):
                src = lax.rem(me_x + k, nx)
                for c in range(2):
                    ref = recv.at[src, pl.ds(c * half_rows, half_rows), pl.ds(local * W, W)]
                    pltpu.make_async_remote_copy(
                        src_ref=ref, dst_ref=ref, send_sem=rs_s.at[0], recv_sem=rs_r.at[src, local, c], **device(sibling),
                    ).wait_recv()

        @pl.loop(0, D // W)
        def _(q):
            owner = lax.div(q, per_owner)

            @pl.when((owner == sibling) & jnp.logical_not(in_tail(q)))
            def _():
                whole_copy(q).wait_send()

            @pl.when(lax.div(owner, nx) != me_x)
            def _():
                pair_copy(q).wait_send()
                half_copy(q).wait_send()

        for j in range(len(relays)):
            @pl.when(is_relay)
            def _():
                relay_copy(j, relay_out).wait_send()

    def wait_sends(slots):
        for s in slots:
            for c in range(chunks(s)):
                for d in range(2):
                    when(live(s, seat[d]), lambda: ring_copy(s, c, d, seat[d]).wait_send())

    def sends_after(s, c):
        if s + 1 < last and slot_tight[s + 1]:
            send(s + 1, c, tight=True)
        if s + 2 < last:
            send(s + 2, c, tight=False if slot_tight[s + 2] else None)
        if (s + 2, c) == (last, 1):
            for e in range(last_chunks):
                send(last, e)

    queue = [[("own", h) for h in range(2)]]
    hidden_from = 2 * max(s for s in range(S) if slot_kinds[s] == "U") + 1
    blocks = F // width
    per_step = (blocks + 1) // 2
    prior = [("none",)] * 2
    normal_at = max(0, hidden_from - 6)

    for s in range(S):
        for c in range(chunks(s)):
            k = index(s, c)
            if s == last:
                if c == 0:
                    wait_sends(range(last - 2))
                    last_slot()
                continue
            arrive(s, c)
            for j, (t, _) in enumerate(relays):
                if t + 1 == s and c == 0:
                    @pl.when(is_relay)
                    def _():
                        relay_copy(j, 1 - relay_out).wait_recv()
                    if j % 2 == 0:
                        queue.append([("relay", j), ("none",)])
                    elif queue and queue[-1][0] == ("relay", j - 1):
                        queue[-1][1] = ("relay", j)
                    else:
                        queue.append([("relay", j), ("none",)])
            sends_after(s, c)
            if c == 1 and s < last:
                for j, (t, _) in enumerate(relays):
                    if t == s + 1:
                        @pl.when(is_relay)
                        def _():
                            relay_copy(j, relay_out).start()
                if slot_kinds[s] == "D":
                    queue.append([("ring", s, d) for d in range(2)])
            if k == normal_at:
                normalise()
            if k in (hidden_from, hidden_from + 1):
                make_hidden((k - hidden_from) * per_step, min(per_step, blocks - (k - hidden_from) * per_step))
            if k > hidden_from + 1 and queue:
                count = len(queue) if (s, c) == (last - 1, 1) else pairs_per_step
                take, queue = queue[:count], queue[count:]
                run_tiles(prior, take)
                prior = take[-1]
                if not queue:
                    final = [entry_of(e) for e in prior]
                    pass_pair([e[0] for e in final], [e[1] for e in final])
                    prior = [("none",)] * 2

    wait_sends(range(last - 2, S))

    @pl.when(tail_on & jnp.logical_not(tail_mine))
    def _():
        for q in tail_q:
            for i in range(2):
                across_copy(q, i).wait_send()

    @pl.when(tail_on & tail_mine)
    def _():
        for q in tail_q:
            for i in range(2):
                across_copy(q, i).wait_recv()


def routed_finish(n_fs, n_tp, up_v, dn_v, recv, hid, up_o, dn_o, mlp_o, total, out, sem):
    n, T, Dk = recv.shape
    W = up_v.shape[0] // n_fs // 2
    per_owner = Dk // W
    copies = []
    for k, (v, o) in enumerate(((up_v, up_o), (dn_v, dn_o))):
        half = v.shape[0] // 2
        copies += [
            pltpu.make_async_copy(v.at[pl.ds(h * half, half), :], o.at[pl.ds(h * half, half), :], sem.at[2 * k + h])
            for h in range(2)
        ]
    for c in copies:
        c.start()
    here = Places(n_fs, n_tp)
    tail_on, tail_q, tail_mine = here.last_tiles(per_owner)
    rows = 128

    @pl.loop(0, T // rows)
    def _(i):
        r = pl.ds(pl.multiple_of(i * rows, rows), rows)
        acc = recv[0, r, :].astype(jnp.float32)
        for k in range(1, n):
            acc += recv[k, r, :].astype(jnp.float32)
        total[r, :] = acc

    @pl.when(tail_on & tail_mine)
    def _():
        @pl.loop(0, 2)
        def _(i):
            r = pl.ds(pl.multiple_of(i * (T // 2), T // 2), T // 2)
            both = jnp.concatenate([dn_v[:, pl.ds(pl.multiple_of(q * W, W), W)] for q in tail_q], axis=1)
            late = jnp.dot(hid[r, :], both, preferred_element_type=jnp.float32).astype(jnp.bfloat16)
            for j, q in enumerate(tail_q):
                cols = pl.ds(pl.multiple_of(lax.rem(q, per_owner) * W, W), W)
                total[r, cols] += late[:, j * W : (j + 1) * W].astype(jnp.float32)

    @pl.loop(0, T // rows)
    def _(i):
        r = pl.ds(pl.multiple_of(i * rows, rows), rows)
        out[r, :] = total[r, :].astype(jnp.bfloat16)

    written = pltpu.make_async_copy(out, mlp_o, sem.at[4])
    written.start()
    for c in copies:
        c.wait()
    written.wait()


def solution(mesh):
    n_fs, n_tp = mesh.shape["fs"], mesh.shape["tp"]
    bf16 = jnp.bfloat16

    def routed(tokens, norm_gain, up_master, down_master):
        T, Dk = tokens.shape
        R, F = up_master.shape
        D, W = n_fs * R, R // 2
        waves = 2 * len(slot_kinds) + last_chunks - 2
        hbm_spec = pl.BlockSpec(memory_space=pltpu.HBM)
        vmem_spec = pl.BlockSpec(memory_space=pltpu.VMEM)
        dma = pltpu.SemaphoreType.DMA
        held = pl.pallas_call(
            functools.partial(routed_kernel, n_fs, n_tp),
            out_shape=(
                pltpu.VMEM((D, F), bf16),
                pltpu.VMEM((F, D), bf16),
                pltpu.VMEM((n_tp // 2 + 1, T, Dk), bf16),
                pltpu.VMEM((T, F), bf16),
            ),
            in_specs=[hbm_spec] * 4,
            out_specs=(vmem_spec,) * 4,
            scratch_shapes=[
                pltpu.VMEM((T, D), bf16),
                pltpu.VMEM((D // W, T, W), bf16),
                pltpu.VMEM((D // W, T // 2, W), bf16),
                pltpu.VMEM((R, F), jnp.float32),
                pltpu.VMEM((R, F), jnp.float32),
                pltpu.VMEM((1, R), jnp.float32),
                pltpu.VMEM((T, 2 * W), jnp.float32),
                dma((7,)),
                dma((n_tp,)),
                dma((n_tp,)),
                dma((2, waves)),
                dma((2, waves)),
                dma((len(relays),)),
                dma((len(relays),)),
                dma((D // W,)),
                dma((D // W,)),
                dma((D // W,)),
                dma((n_tp // 2 + 1, Dk // W, 2)),
            ],
            compiler_params=pltpu.CompilerParams(
                collective_id=0, has_side_effects=True, vmem_limit_bytes=40 * 2**20
            ),
        )(tokens, norm_gain[None, :], up_master, down_master)
        return pl.pallas_call(
            functools.partial(routed_finish, n_fs, n_tp),
            out_shape=(
                jax.ShapeDtypeStruct((D, F), bf16),
                jax.ShapeDtypeStruct((F, D), bf16),
                jax.ShapeDtypeStruct((T, Dk), bf16),
            ),
            in_specs=[vmem_spec] * 4,
            out_specs=(pl.BlockSpec(memory_space=pl.ANY),) * 3,
            scratch_shapes=[pltpu.VMEM((T, Dk), jnp.float32), pltpu.VMEM((T, Dk), bf16), dma((5,))],
            compiler_params=pltpu.CompilerParams(vmem_limit_bytes=12 * 2**20),
        )(*held)

    def on_device(tokens, norm_gain, up_master, down_master):
        T, Dk = tokens.shape
        R, F = up_master.shape
        D = n_fs * R
        W = R // 2 if (R // 2) % 128 == 0 else R
        S = len(send_list(n_fs))
        any_spec = pl.BlockSpec(memory_space=pl.ANY)
        vmem_spec = pl.BlockSpec(memory_space=pltpu.VMEM)
        if (n_fs, grid_of(n_fs)[1], n_tp * grid_of(n_fs)[1], 2 * W) == (ring_places, 2, n_fs, R):
            return routed(tokens, norm_gain, up_master, down_master)
        up_v, dn_v, recv = pl.pallas_call(
            functools.partial(gather_kernel, n_fs, n_tp),
            out_shape=(pltpu.VMEM((D, F), bf16), pltpu.VMEM((F, D), bf16), pltpu.VMEM((n_tp // 2 + 1, T, Dk), bf16)),
            in_specs=[pl.BlockSpec(memory_space=pltpu.HBM)] * 4,
            out_specs=(vmem_spec,) * 3,
            scratch_shapes=[
                pltpu.VMEM((T, D), bf16),
                pltpu.VMEM((T, F), bf16),
                pltpu.VMEM((D // W, T, W), bf16),
                pltpu.VMEM((D // W, T // 2, W), bf16),
                pltpu.VMEM((R, F), jnp.float32),
                pltpu.VMEM((R, F), jnp.float32),
                pltpu.VMEM((1, R), jnp.float32),
                pltpu.SemaphoreType.DMA((4,)),
                pltpu.SemaphoreType.DMA((n_tp,)),
                pltpu.SemaphoreType.DMA((n_tp,)),
                pltpu.SemaphoreType.DMA((2, S)),
                pltpu.SemaphoreType.DMA((2, S)),
                pltpu.SemaphoreType.DMA((D // W,)),
                pltpu.SemaphoreType.DMA((D // W,)),
                pltpu.SemaphoreType.DMA((D // W,)),
                pltpu.SemaphoreType.DMA((n_tp // 2 + 1, Dk // W, 2)),
            ],
            compiler_params=pltpu.CompilerParams(
                collective_id=0, has_side_effects=True, vmem_limit_bytes=44 * 2**20
            ),
        )(tokens, norm_gain[None, :], up_master, down_master)
        return pl.pallas_call(
            finish_kernel,
            out_shape=(
                jax.ShapeDtypeStruct((D, F), bf16),
                jax.ShapeDtypeStruct((F, D), bf16),
                jax.ShapeDtypeStruct((T, Dk), bf16),
            ),
            in_specs=[vmem_spec] * 3,
            out_specs=(any_spec,) * 3,
            scratch_shapes=[pltpu.VMEM((T, Dk), bf16), pltpu.SemaphoreType.DMA((3,))],
            compiler_params=pltpu.CompilerParams(vmem_limit_bytes=8 * 2**20),
        )(up_v, dn_v, recv)

    in_specs = (P("fs", "tp"), P("fs"), P("fs", "tp"), P("fs", "tp"))
    out_specs = (P(None, "tp"), P("tp", None), P("fs", "tp"))
    return jax.shard_map(on_device, mesh=mesh, in_specs=in_specs, out_specs=out_specs, check_vma=False)
```

```python
import functools

import jax
import jax.numpy as jnp
from jax import lax
from jax.experimental import pallas as pl
from jax.experimental.pallas import tpu as pltpu
from jax.sharding import PartitionSpec as P

norm_floor = 1e-06
MESH = pl.DeviceIdType.MESH


def grid_of(n):
    ny = max(d for d in range(1, n + 1) if n % d == 0 and d * d <= n)
    return n // ny, ny


def position_of(f, nz, ny):
    if ny == 1:
        return f
    z, y = lax.div(f, ny), lax.rem(f, ny)
    tail = lax.div(y + (ny - 1), ny)
    k = nz - 1 - z
    odd = lax.rem(k, 2)
    r = (1 - odd) * (y - 1) + odd * (ny - 1 - y)
    return (1 - tail) * z + tail * (nz + k * (ny - 1) + r)


def index_at(p, nz, ny):
    if ny == 1:
        return p
    tail = lax.div(lax.div(p, nz) + (ny - 2), ny - 1)
    q = tail * (p - nz)
    k = lax.div(q, ny - 1)
    r = lax.rem(q, ny - 1)
    odd = lax.rem(k, 2)
    z = (1 - tail) * p + tail * (nz - 1 - k)
    y = tail * ((1 - odd) * (1 + r) + odd * (ny - 1 - r))
    return z * ny + y


def send_list(n):
    hops = n // 2
    split = n % 2 == 0

    def pieces(a, h):
        return [(a, h, 0)] if split and h == hops - 1 else [(a, h, 0), (a, h, 1)]

    ups = [p for h in range(1, hops) for p in pieces("u", h)]
    downs = [p for h in range(1, hops) for p in pieces("d", h)]
    own_u, own_d = pieces("u", 0), pieces("d", 0)
    return own_u + own_d[:1] + ups + own_d[1:] + downs


def gather_kernel(
    n_fs, n_tp, tokens, gain, up_l, dn_l, up_w, dn_w, recv, x, hid, part, stage, up_f, dn_f, gain_v,
    loc_sem, tok_s, tok_r, ring_s, ring_r, pre_s, pre_r, rs_s, rs_r,
):
    nz, ny = grid_of(n_fs)
    me_f, me_t = lax.axis_index("fs"), lax.axis_index("tp")
    pos = position_of(me_f, nz, ny)
    T, Dk = tokens.shape
    R, F = up_l.shape
    D = n_fs * R
    split_cols = (R // 2) % 128 == 0
    W = R // 2 if split_cols else R

    def at(offset):
        return index_at(lax.rem(pos + offset + n_fs, n_fs), nz, ny)

    right, left = at(1), at(-1)

    def tp_peer(k):
        return lax.rem(me_t + k, n_tp)

    barrier = pltpu.get_barrier_semaphore()
    for f in (right, left):
        pl.semaphore_signal(barrier, inc=1, device_id={"fs": f, "tp": me_t}, device_id_type=MESH)
    for k in range(1, n_tp):
        pl.semaphore_signal(barrier, inc=1, device_id={"fs": me_f, "tp": tp_peer(k)}, device_id_type=MESH)

    def up_piece(f, h):
        return up_w.at[pl.ds(pl.multiple_of(f * R + h * (R // 2), R // 2), R // 2), :]

    def dn_piece(f, h):
        if split_cols:
            return dn_w.at[:, pl.ds(pl.multiple_of(f * R + h * (R // 2), R // 2), R // 2)]
        return dn_w.at[pl.ds(h * (F // 2), F // 2), pl.ds(pl.multiple_of(f * R, R), R)]

    def tok_cols(t):
        return x.at[:, pl.ds(pl.multiple_of(t * Dk, Dk), Dk)]

    own = [
        pltpu.make_async_copy(up_l, up_f, loc_sem.at[0]),
        pltpu.make_async_copy(tokens, tok_cols(me_t), loc_sem.at[1]),
        pltpu.make_async_copy(dn_l, dn_f, loc_sem.at[2]),
    ]
    gain_copy = pltpu.make_async_copy(gain, gain_v, loc_sem.at[3])
    for c in [gain_copy] + own:
        c.start()
    own_rows = pl.ds(pl.multiple_of(me_f * R, R), R)
    gain_copy.wait()
    spread = jnp.transpose(jnp.broadcast_to(gain_v[...], (128, R)))
    own[0].wait()
    for c in range(F // 128):
        cols = pl.ds(c * 128, 128)
        up_w[own_rows, cols] = (spread * up_f[:, cols]).astype(jnp.bfloat16)
    own[1].wait()
    pl.semaphore_wait(barrier, n_tp + 1)

    order = send_list(n_fs)
    S = len(order)

    def ring_copy(s, d):
        a, hop, second = order[s]
        half = second if d == 0 else 1 - second
        f = at(-hop if d == 0 else hop)
        ref = up_piece(f, half) if a == "u" else dn_piece(f, half)
        return pltpu.make_async_remote_copy(
            src_ref=ref, dst_ref=ref, send_sem=ring_s.at[d, s], recv_sem=ring_r.at[d, s],
            device_id={"fs": right if d == 0 else left, "tp": me_t}, device_id_type=MESH,
        )

    def arrival(s, d):
        a, hop, second = order[s]
        half = second if d == 0 else 1 - second
        f = at(-(hop + 1) if d == 0 else hop + 1)
        return f, half, (up_piece(f, half) if a == "u" else dn_piece(f, half))

    def wait_arrival(s, d):
        f, half, ref = arrival(s, d)
        pltpu.make_async_remote_copy(
            src_ref=ref, dst_ref=ref, send_sem=ring_s.at[d, s], recv_sem=ring_r.at[d, s],
            device_id={"fs": right if d == 0 else left, "tp": me_t}, device_id_type=MESH,
        ).wait_recv()

    needs = [-1 if hop == 0 else order.index((a, hop - 1, second)) for a, hop, second in order]
    issued = [0]

    def issue(upto):
        while issued[0] < S and needs[issued[0]] <= upto:
            if upto < 0 and issued[0] >= 3:
                break
            for d in range(2):
                ring_copy(issued[0], d).start()
            issued[0] += 1

    for s in range(2):
        for d in range(2):
            ring_copy(s, d).start()

    def token_copy(k):
        return pltpu.make_async_remote_copy(
            src_ref=tok_cols(me_t), dst_ref=tok_cols(me_t), send_sem=tok_s.at[k], recv_sem=tok_r.at[k],
            device_id={"fs": me_f, "tp": tp_peer(k)}, device_id_type=MESH,
        )

    for k in range(1, n_tp):
        token_copy(k).start()
    own[2].wait()
    block = min(F, 256)

    @pl.loop(0, F // block)
    def _(i):
        r = pl.ds(pl.multiple_of(i * block, block), block)
        dn_w[r, own_rows] = jnp.transpose(dn_f[:, r]).astype(jnp.bfloat16)

    issued[0] = 2
    issue(-1)

    def normalise():
        for k in range(1, n_tp):
            src = lax.rem(me_t - k + n_tp, n_tp)
            pltpu.make_async_remote_copy(
                src_ref=tok_cols(src), dst_ref=tok_cols(src), send_sem=tok_s.at[k], recv_sem=tok_r.at[k],
                device_id={"fs": me_f, "tp": tp_peer(k)}, device_id_type=MESH,
            ).wait_recv()
            token_copy(k).wait_send()
        rows = 64

        @pl.loop(0, T // rows)
        def _(i):
            r = pl.ds(pl.multiple_of(i * rows, rows), rows)
            v = x[r, :].astype(jnp.float32)
            x[r, :] = (v * lax.rsqrt(jnp.mean(v * v, axis=-1, keepdims=True) + norm_floor)).astype(jnp.bfloat16)

    def make_hidden():
        width = 256

        @pl.loop(0, F // width)
        def _(i):
            c = pl.ds(pl.multiple_of(i * width, width), width)
            pre = jnp.dot(x[...], up_w[:, c], preferred_element_type=jnp.float32)
            hid[:, c] = jnp.square(jnp.maximum(pre, 0.0)).astype(jnp.bfloat16)

    per_owner = Dk // W
    nx = n_tp // 2
    half_rows = T // 2
    me_x, me_c = lax.div(me_t, 2), lax.rem(me_t, 2)
    sibling = me_t + 1 - 2 * me_c
    my_half = pl.ds(pl.multiple_of(me_c * half_rows, half_rows), half_rows)
    its_half = pl.ds(pl.multiple_of((1 - me_c) * half_rows, half_rows), half_rows)

    def device(t):
        return dict(device_id={"fs": me_f, "tp": t}, device_id_type=MESH)

    def cols_of(q):
        return pl.ds(pl.multiple_of(lax.rem(q, per_owner) * W, W), W)

    def whole_copy(q):
        return pltpu.make_async_remote_copy(
            src_ref=part.at[q], dst_ref=recv.at[nx, :, cols_of(q)],
            send_sem=rs_s.at[q], recv_sem=rs_r.at[nx, lax.rem(q, per_owner), 0], **device(sibling),
        )

    def pair_copy(q):
        return pltpu.make_async_remote_copy(
            src_ref=part.at[q, its_half], dst_ref=stage.at[q],
            send_sem=pre_s.at[q], recv_sem=pre_r.at[q], **device(sibling),
        )

    def half_copy(q):
        return pltpu.make_async_remote_copy(
            src_ref=part.at[q, my_half], dst_ref=recv.at[me_x, my_half, cols_of(q)],
            send_sem=rs_s.at[q], recv_sem=rs_r.at[me_x, lax.rem(q, per_owner), me_c],
            **device(lax.div(q, per_owner)),
        )

    def pass_on(q):
        @pl.when(lax.div(q, 2 * per_owner) != me_x)
        def _():
            pair_copy(q).wait_recv()
            both = part[q, my_half, :].astype(jnp.float32) + stage[q].astype(jnp.float32)
            part[q, my_half, :] = both.astype(jnp.bfloat16)
            half_copy(q).start()

    def do_parts(first, count):
        c = pl.ds(pl.multiple_of(first * W, W), count * W)

        @pl.loop(0, 2)
        def _(i):
            r = pl.ds(pl.multiple_of(lax.rem(i + 1 + me_c, 2) * half_rows, half_rows), half_rows)
            out = jnp.dot(hid[r, :], dn_w[:, c], preferred_element_type=jnp.float32).astype(jnp.bfloat16)
            for k in range(count):
                part[first + k, r, :] = out[:, k * W : (k + 1) * W]
            for k in range(count):
                owner = lax.div(first + k, per_owner)

                @pl.when((i == 0) & (lax.div(owner, 2) != me_x))
                def _():
                    pair_copy(first + k).start()

                @pl.when((i == 1) & (owner == sibling))
                def _():
                    whole_copy(first + k).start()

    per_chunk = R // W
    ready = [(me_f * per_chunk, per_chunk)]
    last_up = max(s for s in range(S) if order[s][0] == "u")
    norm_at = max(0, last_up - 2)
    for s in range(S):
        for d in range(2):
            wait_arrival(s, d)
        issue(s)
        a, hop, _ = order[s]
        if a == "d" and split_cols:
            if n_fs % 2 == 0 and hop == n_fs // 2 - 1:
                ready.append((at(hop + 1) * 2, 2))
            else:
                for d in range(2):
                    f, half, _ = arrival(s, d)
                    ready.append((f * 2 + half, 1))
        if s == norm_at:
            normalise()
        if s == last_up:
            make_hidden()
        if s >= last_up:
            for first, count in ready:
                do_parts(first, count)
            for first, count in ready:
                for k in range(count):
                    pass_on(first + k)
            ready = []
    if not split_cols:
        @pl.loop(0, n_fs)
        def _(q):
            @pl.when(q != me_f)
            def _():
                do_parts(q, 1)
                pass_on(q)

    @pl.loop(0, per_owner)
    def _(local):
        cols = pl.ds(pl.multiple_of(local * W, W), W)
        recv[me_x, :, cols] = part[me_t * per_owner + local]

    for d in range(2):
        for s in range(S):
            ring_copy(s, d).wait_send()

    @pl.loop(0, D // W)
    def _(q):
        owner = lax.div(q, per_owner)

        @pl.when(owner == sibling)
        def _():
            whole_copy(q).wait_send()

        @pl.when(lax.div(owner, 2) != me_x)
        def _():
            pair_copy(q).wait_send()
            half_copy(q).wait_send()

    for local in range(per_owner):
        q = me_t * per_owner + local
        whole_copy(q).wait_recv()
        for k in range(1, nx):
            src = lax.rem(me_x + k, nx)
            for c in range(2):
                ref = recv.at[src, pl.ds(c * half_rows, half_rows), pl.ds(local * W, W)]
                pltpu.make_async_remote_copy(
                    src_ref=ref, dst_ref=ref, send_sem=rs_s.at[0], recv_sem=rs_r.at[src, local, c], **device(sibling),
                ).wait_recv()


def finish_kernel(up_v, dn_v, recv, up_o, dn_o, mlp_o, total, sem):
    copies = [pltpu.make_async_copy(up_v, up_o, sem.at[0]), pltpu.make_async_copy(dn_v, dn_o, sem.at[1])]
    for c in copies:
        c.start()
    n, T, _ = recv.shape
    rows = 128

    @pl.loop(0, T // rows)
    def _(i):
        r = pl.ds(pl.multiple_of(i * rows, rows), rows)
        acc = recv[0, r, :].astype(jnp.float32)
        for k in range(1, n):
            acc += recv[k, r, :].astype(jnp.float32)
        total[r, :] = acc.astype(jnp.bfloat16)

    last = pltpu.make_async_copy(total, mlp_o, sem.at[2])
    last.start()
    for c in copies:
        c.wait()
    last.wait()


slot_kinds = "UUDUUDUUUDDDDD"
slot_pieces = (
    0xECA86420, 0xFDB97531,
    0xECA86420, 0xCA86420E,
    0xDB97531F, 0xFAB97531,
    0xA86420EC, 0xB97531FD,
    0x86420ECA, 0xAB97420E,
    0xB986531F, 0x987420EA,
    0x826531F0, 0xCD020EC0,
)
slot_live = (0xFF, 0xFF, 0xFF, 0xFF, 0xFF, 0xFF, 0xFF, 0xFF, 0xFF, 0xFF, 0xFF, 0xFF, 0xFE, 0xDE)
slot_tight = (0x00, 0x00, 0x00, 0x00, 0x00, 0x00, 0x00, 0x00, 0x00, 0x00, 0xC0, 0xC0, 0x80, 0x00)
relays = ((1, 12), (2, 13), (7, 11))
relay_place = 6
ring_places = 8
last_chunks = 4
second_leads = 0x0C
pairs_per_step = 2


def look(word, place, width):
    word = word - 2**32 if word >= 2**31 else word
    return lax.bitwise_and(lax.shift_right_logical(jnp.int32(word), place * width), jnp.int32(2**width - 1))


class Places:
    def __init__(self, n_fs, n_tp):
        nz, ny = grid_of(n_fs)
        self.n, self.nz, self.ny = n_fs, nz, ny
        self.me_f, self.me_t = lax.axis_index("fs"), lax.axis_index("tp")
        self.me_x, self.me_c = lax.div(self.me_t, 2), lax.rem(self.me_t, 2)
        z, y = lax.div(self.me_f, ny), lax.rem(self.me_f, ny)
        along = z + self.me_x * (nz - 1 - 2 * z)
        self.pos = along + y * (n_fs - 1 - 2 * along)
        self.seat = (self.pos, n_fs - 1 - self.pos)
        self.behind = tuple(lax.rem(p + n_fs - 1, n_fs) for p in self.seat)

    def at(self, p):
        side = lax.div(p, self.nz)
        along = p + side * (self.n - 1 - 2 * p)
        return (along + self.me_x * (self.nz - 1 - 2 * along)) * self.ny + side

    def mirrored(self, code, m):
        src, half = lax.div(code, 2), lax.rem(code, 2)
        return self.at(src + m * (self.n - 1 - 2 * src)), half + m * (1 - 2 * half)

    def piece(self, s, place, d):
        return self.mirrored(look(slot_pieces[s], place, 4), d)

    def live(self, s, place):
        return None if slot_live[s] == 2**self.n - 1 else look(slot_live[s], place, 1) == 1

    def last_tiles(self, per_owner):
        last = len(slot_kinds) - 1
        tiles = []
        for d in range(2):
            f, half = self.piece(last, self.behind[d], d)
            tiles.append(f * 2 + half)
        return self.live(last, self.behind[0]), tiles, lax.div(tiles[0], per_owner) == self.me_t


def routed_kernel(
    n_fs, n_tp, tokens, gain, up_l, dn_l, up_w, dn_w, recv, hid, x, part, stage, up_f, dn_f, gain_v, acc,
    loc_sem, tok_s, tok_r, ring_s, ring_r, y_s, y_r, pre_s, pre_r, rs_s, rs_r,
):
    R, F = up_l.shape
    W = R // 2
    quarter = W // 2
    gain_copy = pltpu.make_async_copy(gain, gain_v, loc_sem.at[0])
    firsts = [(h, c) for c in range(2) for h in range(2)]

    def up_copy(h, c):
        rows = pl.ds(h * W + c * quarter, quarter)
        return pltpu.make_async_copy(up_l.at[rows, :], up_f.at[rows, :], loc_sem.at[1 + 2 * h + c])

    gain_copy.start()
    for h, c in firsts:
        up_copy(h, c).start()

    here = Places(n_fs, n_tp)
    me_f, me_t, me_x, me_c, pos, at = here.me_f, here.me_t, here.me_x, here.me_c, here.pos, here.at
    seat, behind, mirrored, piece, live = here.seat, here.behind, here.mirrored, here.piece, here.live
    T, Dk = tokens.shape
    R, F = up_l.shape
    D = n_fs * R
    W = R // 2
    nx = n_tp // 2
    sibling = me_t + 1 - 2 * me_c
    half_rows = T // 2
    per_owner = Dk // W
    S = len(slot_kinds)
    last = S - 1

    right, left, across = at(lax.rem(pos + 1, n_fs)), at(lax.rem(pos + n_fs - 1, n_fs)), at(n_fs - 1 - pos)
    is_relay = (pos == relay_place) | (pos == n_fs - 1 - relay_place)

    def tp_peer(k):
        return lax.rem(me_t + k, n_tp)

    barrier = pltpu.get_barrier_semaphore()
    for f in (right, left, across):
        pl.semaphore_signal(barrier, inc=1, device_id={"fs": f, "tp": me_t}, device_id_type=MESH)
    for k in range(1, n_tp):
        pl.semaphore_signal(barrier, inc=1, device_id={"fs": me_f, "tp": tp_peer(k)}, device_id_type=MESH)

    def tok_cols(t):
        return x.at[:, pl.ds(pl.multiple_of(t * Dk, Dk), Dk)]

    tok_copy = pltpu.make_async_copy(tokens, tok_cols(me_t), loc_sem.at[5])
    dn_copy = pltpu.make_async_copy(dn_l, dn_f, loc_sem.at[6])

    def when(pred, body):
        if pred is None:
            body()
        else:
            pl.when(pred)(body)

    def chunks(s):
        return last_chunks if s == last else 2

    def index(s, c):
        return 2 * s + c

    def ref_of(kind, f, half, c, n):
        if kind == "U":
            rows = W // n
            return up_w.at[pl.ds(pl.multiple_of(f * R + half * W + c * rows, rows), rows), :]
        return dn_w.at[pl.ds(c * (F // n), F // n), pl.ds(pl.multiple_of(f * R + half * W, W), W)]

    def ring_copy(s, c, d, place):
        f, half = piece(s, place, d)
        ref = ref_of(slot_kinds[s], f, half, c, chunks(s))
        return pltpu.make_async_remote_copy(
            src_ref=ref, dst_ref=ref, send_sem=ring_s.at[d, index(s, c)], recv_sem=ring_r.at[d, index(s, c)],
            device_id={"fs": right if d == 0 else left, "tp": me_t}, device_id_type=MESH,
        )

    def send(s, c, sides=(0, 1), tight=None):
        for d in sides:
            pred = live(s, seat[d])
            if tight is not None:
                here_tight = (look(slot_tight[s], seat[d], 1) == 1) == tight
                pred = here_tight if pred is None else pred & here_tight
            when(pred, lambda: ring_copy(s, c, d, seat[d]).start())

    def arrive(s, c):
        for d in range(2):
            when(live(s, behind[d]), lambda: ring_copy(s, c, d, behind[d]).wait_recv())

    def relay_copy(j, m):
        f, half = mirrored(jnp.int32(relays[j][1]), m)
        ref = ref_of("D", f, half, 0, 1)
        return pltpu.make_async_remote_copy(
            src_ref=ref, dst_ref=ref, send_sem=y_s.at[j], recv_sem=y_r.at[j],
            device_id={"fs": across, "tp": me_t}, device_id_type=MESH,
        )

    relay_out = jnp.where(pos == relay_place, 0, 1)

    own_row = pl.multiple_of(me_f * R, R)
    early_core = jnp.where(me_c == me_x, 0, 1)
    leads = [look(second_leads, seat[d], 1) == early_core for d in range(2)]
    gain_copy.wait()
    spread = jnp.transpose(jnp.broadcast_to(gain_v[...], (128, R)))

    def convert(h, c):
        up_copy(h, c).wait()
        first = h * W + c * quarter
        for j in range(F // 128):
            cols = pl.ds(j * 128, 128)
            up_w[pl.ds(own_row + first, quarter), cols] = (
                spread[first : first + quarter] * up_f[pl.ds(first, quarter), cols]
            ).astype(jnp.bfloat16)

    for h, c in firsts:
        convert(h, c)
        if (h, c) == (0, 0):
            pl.semaphore_wait(barrier, n_tp + 2)
        pl.when(leads[h])(lambda: send(0, c, (h,)))
        if (h, c) == (1, 0):
            tok_copy.start()
            dn_copy.start()
    for d in range(2):
        @pl.when(leads[d])
        def _():
            for e in range(2):
                send(1, e, (d,))

    def token_copy(k):
        return pltpu.make_async_remote_copy(
            src_ref=tok_cols(me_t), dst_ref=tok_cols(me_t), send_sem=tok_s.at[k], recv_sem=tok_r.at[k],
            device_id={"fs": me_f, "tp": tp_peer(k)}, device_id_type=MESH,
        )

    tok_copy.wait()
    for k in range(1, n_tp):
        token_copy(k).start()
    dn_copy.wait()
    block = min(F, 256)

    @pl.loop(0, 2 * (F // block))
    def _(i):
        r = pl.ds(pl.multiple_of(lax.rem(i, F // block) * block, block), block)
        dn_w[r, pl.ds(own_row, R)] = jnp.transpose(dn_f[:, r]).astype(jnp.bfloat16)

    for d in range(2):
        @pl.when(jnp.logical_not(leads[d]))
        def _():
            for t in range(2):
                for e in range(2):
                    send(t, e, (d,))

    def normalise():
        for k in range(1, n_tp):
            src = lax.rem(me_t - k + n_tp, n_tp)
            pltpu.make_async_remote_copy(
                src_ref=tok_cols(src), dst_ref=tok_cols(src), send_sem=tok_s.at[k], recv_sem=tok_r.at[k],
                device_id={"fs": me_f, "tp": tp_peer(k)}, device_id_type=MESH,
            ).wait_recv()
            token_copy(k).wait_send()
        rows = 64

        @pl.loop(0, T // rows)
        def _(i):
            r = pl.ds(pl.multiple_of(i * rows, rows), rows)
            v = x[r, :].astype(jnp.float32)
            x[r, :] = (v * lax.rsqrt(jnp.mean(v * v, axis=-1, keepdims=True) + norm_floor)).astype(jnp.bfloat16)

    width = 256

    def make_hidden(first, count):
        @pl.loop(first, first + count)
        def _(i):
            c = pl.ds(pl.multiple_of(i * width, width), width)
            pre = jnp.dot(x[...], up_w[:, c], preferred_element_type=jnp.float32)
            hid[:, c] = jnp.square(jnp.maximum(pre, 0.0)).astype(jnp.bfloat16)

    my_half = pl.ds(pl.multiple_of(me_c * half_rows, half_rows), half_rows)
    its_half = pl.ds(pl.multiple_of((1 - me_c) * half_rows, half_rows), half_rows)

    def device(t):
        return dict(device_id={"fs": me_f, "tp": t}, device_id_type=MESH)

    def cols_of(q):
        return pl.ds(pl.multiple_of(lax.rem(q, per_owner) * W, W), W)

    def tile(q):
        return pl.ds(pl.multiple_of(q * W, W), W)

    def whole_copy(q):
        return pltpu.make_async_remote_copy(
            src_ref=part.at[q], dst_ref=recv.at[nx, :, cols_of(q)],
            send_sem=rs_s.at[q], recv_sem=rs_r.at[nx, lax.rem(q, per_owner), 0], **device(sibling),
        )

    def pair_copy(q):
        return pltpu.make_async_remote_copy(
            src_ref=part.at[q, its_half], dst_ref=stage.at[q],
            send_sem=pre_s.at[q], recv_sem=pre_r.at[q], **device(sibling),
        )

    def half_copy(q):
        return pltpu.make_async_remote_copy(
            src_ref=part.at[q, my_half], dst_ref=recv.at[me_x, my_half, cols_of(q)],
            send_sem=rs_s.at[q], recv_sem=rs_r.at[me_x, lax.rem(q, per_owner), me_c],
            **device(lax.div(q, per_owner)),
        )

    def pass_on(q):
        @pl.when(lax.div(q, 2 * per_owner) != me_x)
        def _():
            pair_copy(q).wait_recv()
            both = part[q, my_half, :].astype(jnp.float32) + stage[q].astype(jnp.float32)
            part[q, my_half, :] = both.astype(jnp.bfloat16)
            half_copy(q).start()

    def do_pair(q, ok):
        use = [jnp.where(ok[0] == 1, q[0], q[1]), jnp.where(ok[1] == 1, q[1], q[0])]

        @pl.loop(0, 2)
        def _(i):
            r = pl.ds(pl.multiple_of(lax.rem(i + 1 + me_c, 2) * half_rows, half_rows), half_rows)
            both = jnp.concatenate([dn_w[:, tile(u)] for u in use], axis=1)
            out = jnp.dot(hid[r, :], both, preferred_element_type=jnp.float32).astype(jnp.bfloat16)
            for j in range(2):
                owner = lax.div(q[j], per_owner)

                @pl.when(ok[j] == 1)
                def _():
                    part[q[j], r, :] = out[:, j * W : (j + 1) * W]

                    @pl.when((i == 0) & (lax.div(owner, nx) != me_x))
                    def _():
                        pair_copy(q[j]).start()

                    @pl.when((i == 1) & (owner == sibling))
                    def _():
                        whole_copy(q[j]).start()

    def entry_of(e):
        kind = e[0]
        if kind == "none":
            return jnp.int32(0), jnp.int32(0)
        if kind == "own":
            return me_f * 2 + e[1], jnp.int32(1)
        if kind == "relay":
            f, half = mirrored(jnp.int32(relays[e[1]][1]), 1 - relay_out)
            return f * 2 + half, jnp.where(is_relay, 1, 0)
        s, d = e[1], e[2]
        f, half = piece(s, behind[d], d)
        ok = jnp.int32(1) if slot_live[s] == 2**n_fs - 1 else look(slot_live[s], behind[d], 1)
        return f * 2 + half, ok

    def pick(i, values):
        out = values[0]
        for k in range(1, len(values)):
            out = jnp.where(i == k, values[k], out)
        return out

    def pass_pair(q, ok):
        for j in range(2):
            @pl.when(ok[j] == 1)
            def _():
                pass_on(q[j])

    def run_tiles(before, pairs):
        cur = [[entry_of(e) for e in pair] for pair in pairs]
        prev = [[entry_of(e) for e in before]] + cur[:-1]

        @pl.loop(0, len(pairs))
        def _(i):
            def chosen(table, j, what):
                return pick(i, [pair[j][what] for pair in table])

            q, ok = [[chosen(cur, j, what) for j in range(2)] for what in range(2)]

            @pl.when(ok[0] + ok[1] > 0)
            def _():
                do_pair(q, ok)

            pass_pair(*[[chosen(prev, j, what) for j in range(2)] for what in range(2)])

    tail_on, tail_q, tail_mine = here.last_tiles(per_owner)
    depth = F // last_chunks

    def across_copy(q, i):
        r = pl.ds(i * half_rows, half_rows)
        return pltpu.make_async_remote_copy(
            src_ref=part.at[q, r], dst_ref=recv.at[nx, r, cols_of(q)],
            send_sem=(rs_s, pre_s)[i].at[q], recv_sem=rs_r.at[nx, lax.rem(q, per_owner), i], **device(sibling),
        )

    def last_slot():
        for c in range(last_chunks):
            k = pl.ds(c * depth, depth)
            @pl.when(tail_on & jnp.logical_not(tail_mine))
            def _():
                for d in range(2):
                    ring_copy(last, c, d, behind[d]).wait_recv()
                for i in range(2):
                    r = pl.ds(i * half_rows, half_rows)
                    both = jnp.concatenate([dn_w[k, tile(q)] for q in tail_q], axis=1)
                    out = jnp.dot(hid[r, k], both, preferred_element_type=jnp.float32)
                    if c > 0:
                        out += acc[r, :]
                    if c < last_chunks - 1:
                        acc[r, :] = out
                    else:
                        for j, q in enumerate(tail_q):
                            part[q, r, :] = out[:, j * W : (j + 1) * W].astype(jnp.bfloat16)
                        for q in tail_q:
                            across_copy(q, i).start()

        settle()
        wait_sends(range(last - 2, last))

        @pl.when(tail_on & tail_mine)
        def _():
            for c in range(last_chunks):
                for d in range(2):
                    ring_copy(last, c, d, behind[d]).wait_recv()

    def in_tail(q):
        return tail_on & ((q == tail_q[0]) | (q == tail_q[1]))

    def settle():
        @pl.loop(0, per_owner)
        def _(local):
            q = me_t * per_owner + local

            @pl.when(jnp.logical_not(in_tail(q)))
            def _():
                recv[me_x, :, cols_of(q)] = part[q]
                whole_copy(q).wait_recv()

            @pl.when(in_tail(q))
            def _():
                recv[me_x, :, cols_of(q)] = jnp.zeros((T, W), jnp.bfloat16)

        for local in range(per_owner):
            for k in range(1, nx):
                src = lax.rem(me_x + k, nx)
                for c in range(2):
                    ref = recv.at[src, pl.ds(c * half_rows, half_rows), pl.ds(local * W, W)]
                    pltpu.make_async_remote_copy(
                        src_ref=ref, dst_ref=ref, send_sem=rs_s.at[0], recv_sem=rs_r.at[src, local, c], **device(sibling),
                    ).wait_recv()

        @pl.loop(0, D // W)
        def _(q):
            owner = lax.div(q, per_owner)

            @pl.when((owner == sibling) & jnp.logical_not(in_tail(q)))
            def _():
                whole_copy(q).wait_send()

            @pl.when(lax.div(owner, nx) != me_x)
            def _():
                pair_copy(q).wait_send()
                half_copy(q).wait_send()

        for j in range(len(relays)):
            @pl.when(is_relay)
            def _():
                relay_copy(j, relay_out).wait_send()

    def wait_sends(slots):
        for s in slots:
            for c in range(chunks(s)):
                for d in range(2):
                    when(live(s, seat[d]), lambda: ring_copy(s, c, d, seat[d]).wait_send())

    def sends_after(s, c):
        if s + 1 < last and slot_tight[s + 1]:
            send(s + 1, c, tight=True)
        if s + 2 < last:
            send(s + 2, c, tight=False if slot_tight[s + 2] else None)
        if (s + 2, c) == (last, 1):
            for e in range(last_chunks):
                send(last, e)

    queue = [[("own", h) for h in range(2)]]
    hidden_from = 2 * max(s for s in range(S) if slot_kinds[s] == "U") + 1
    blocks = F // width
    per_step = (blocks + 1) // 2
    prior = [("none",)] * 2
    normal_at = max(0, hidden_from - 6)

    for s in range(S):
        for c in range(chunks(s)):
            k = index(s, c)
            if s == last:
                if c == 0:
                    wait_sends(range(last - 2))
                    last_slot()
                continue
            arrive(s, c)
            for j, (t, _) in enumerate(relays):
                if t + 1 == s and c == 0:
                    @pl.when(is_relay)
                    def _():
                        relay_copy(j, 1 - relay_out).wait_recv()
                    if j % 2 == 0:
                        queue.append([("relay", j), ("none",)])
                    elif queue and queue[-1][0] == ("relay", j - 1):
                        queue[-1][1] = ("relay", j)
                    else:
                        queue.append([("relay", j), ("none",)])
            sends_after(s, c)
            if c == 1 and s < last:
                for j, (t, _) in enumerate(relays):
                    if t == s + 1:
                        @pl.when(is_relay)
                        def _():
                            relay_copy(j, relay_out).start()
                if slot_kinds[s] == "D":
                    queue.append([("ring", s, d) for d in range(2)])
            if k == normal_at:
                normalise()
            if k in (hidden_from, hidden_from + 1):
                make_hidden((k - hidden_from) * per_step, min(per_step, blocks - (k - hidden_from) * per_step))
            if k > hidden_from + 1 and queue:
                count = len(queue) if (s, c) == (last - 1, 1) else pairs_per_step
                take, queue = queue[:count], queue[count:]
                run_tiles(prior, take)
                prior = take[-1]
                if not queue:
                    final = [entry_of(e) for e in prior]
                    pass_pair([e[0] for e in final], [e[1] for e in final])
                    prior = [("none",)] * 2

    wait_sends((last,))

    @pl.when(tail_on & jnp.logical_not(tail_mine))
    def _():
        for q in tail_q:
            for i in range(2):
                across_copy(q, i).wait_send()

    @pl.when(tail_on & tail_mine)
    def _():
        for q in tail_q:
            for i in range(2):
                across_copy(q, i).wait_recv()


def routed_finish(n_fs, n_tp, up_v, dn_v, recv, hid, up_o, dn_o, mlp_o, total, out, sem):
    n, T, Dk = recv.shape
    W = up_v.shape[0] // n_fs // 2
    per_owner = Dk // W
    copies = []
    for k, (v, o) in enumerate(((up_v, up_o), (dn_v, dn_o))):
        half = v.shape[0] // 2
        copies += [
            pltpu.make_async_copy(v.at[pl.ds(h * half, half), :], o.at[pl.ds(h * half, half), :], sem.at[2 * k + h])
            for h in range(2)
        ]
    for c in copies:
        c.start()
    here = Places(n_fs, n_tp)
    tail_on, tail_q, tail_mine = here.last_tiles(per_owner)
    rows = 128

    @pl.loop(0, T // rows)
    def _(i):
        r = pl.ds(pl.multiple_of(i * rows, rows), rows)
        acc = recv[0, r, :].astype(jnp.float32)
        for k in range(1, n):
            acc += recv[k, r, :].astype(jnp.float32)
        total[r, :] = acc

    @pl.when(tail_on & tail_mine)
    def _():
        @pl.loop(0, 2)
        def _(i):
            r = pl.ds(pl.multiple_of(i * (T // 2), T // 2), T // 2)
            both = jnp.concatenate([dn_v[:, pl.ds(pl.multiple_of(q * W, W), W)] for q in tail_q], axis=1)
            late = jnp.dot(hid[r, :], both, preferred_element_type=jnp.float32).astype(jnp.bfloat16)
            for j, q in enumerate(tail_q):
                cols = pl.ds(pl.multiple_of(lax.rem(q, per_owner) * W, W), W)
                total[r, cols] += late[:, j * W : (j + 1) * W].astype(jnp.float32)

    @pl.loop(0, T // rows)
    def _(i):
        r = pl.ds(pl.multiple_of(i * rows, rows), rows)
        out[r, :] = total[r, :].astype(jnp.bfloat16)

    written = pltpu.make_async_copy(out, mlp_o, sem.at[4])
    written.start()
    for c in copies:
        c.wait()
    written.wait()


def solution(mesh):
    n_fs, n_tp = mesh.shape["fs"], mesh.shape["tp"]
    bf16 = jnp.bfloat16

    def routed(tokens, norm_gain, up_master, down_master):
        T, Dk = tokens.shape
        R, F = up_master.shape
        D, W = n_fs * R, R // 2
        waves = 2 * len(slot_kinds) + last_chunks - 2
        hbm_spec = pl.BlockSpec(memory_space=pltpu.HBM)
        vmem_spec = pl.BlockSpec(memory_space=pltpu.VMEM)
        dma = pltpu.SemaphoreType.DMA
        held = pl.pallas_call(
            functools.partial(routed_kernel, n_fs, n_tp),
            out_shape=(
                pltpu.VMEM((D, F), bf16),
                pltpu.VMEM((F, D), bf16),
                pltpu.VMEM((n_tp // 2 + 1, T, Dk), bf16),
                pltpu.VMEM((T, F), bf16),
            ),
            in_specs=[hbm_spec] * 4,
            out_specs=(vmem_spec,) * 4,
            scratch_shapes=[
                pltpu.VMEM((T, D), bf16),
                pltpu.VMEM((D // W, T, W), bf16),
                pltpu.VMEM((D // W, T // 2, W), bf16),
                pltpu.VMEM((R, F), jnp.float32),
                pltpu.VMEM((R, F), jnp.float32),
                pltpu.VMEM((1, R), jnp.float32),
                pltpu.VMEM((T, 2 * W), jnp.float32),
                dma((7,)),
                dma((n_tp,)),
                dma((n_tp,)),
                dma((2, waves)),
                dma((2, waves)),
                dma((len(relays),)),
                dma((len(relays),)),
                dma((D // W,)),
                dma((D // W,)),
                dma((D // W,)),
                dma((n_tp // 2 + 1, Dk // W, 2)),
            ],
            compiler_params=pltpu.CompilerParams(
                collective_id=0, has_side_effects=True, vmem_limit_bytes=40 * 2**20
            ),
        )(tokens, norm_gain[None, :], up_master, down_master)
        return pl.pallas_call(
            functools.partial(routed_finish, n_fs, n_tp),
            out_shape=(
                jax.ShapeDtypeStruct((D, F), bf16),
                jax.ShapeDtypeStruct((F, D), bf16),
                jax.ShapeDtypeStruct((T, Dk), bf16),
            ),
            in_specs=[vmem_spec] * 4,
            out_specs=(pl.BlockSpec(memory_space=pl.ANY),) * 3,
            scratch_shapes=[pltpu.VMEM((T, Dk), jnp.float32), pltpu.VMEM((T, Dk), bf16), dma((5,))],
            compiler_params=pltpu.CompilerParams(vmem_limit_bytes=12 * 2**20),
        )(*held)

    def on_device(tokens, norm_gain, up_master, down_master):
        T, Dk = tokens.shape
        R, F = up_master.shape
        D = n_fs * R
        W = R // 2 if (R // 2) % 128 == 0 else R
        S = len(send_list(n_fs))
        any_spec = pl.BlockSpec(memory_space=pl.ANY)
        vmem_spec = pl.BlockSpec(memory_space=pltpu.VMEM)
        if (n_fs, grid_of(n_fs)[1], n_tp * grid_of(n_fs)[1], 2 * W) == (ring_places, 2, n_fs, R):
            return routed(tokens, norm_gain, up_master, down_master)
        up_v, dn_v, recv = pl.pallas_call(
            functools.partial(gather_kernel, n_fs, n_tp),
            out_shape=(pltpu.VMEM((D, F), bf16), pltpu.VMEM((F, D), bf16), pltpu.VMEM((n_tp // 2 + 1, T, Dk), bf16)),
            in_specs=[pl.BlockSpec(memory_space=pltpu.HBM)] * 4,
            out_specs=(vmem_spec,) * 3,
            scratch_shapes=[
                pltpu.VMEM((T, D), bf16),
                pltpu.VMEM((T, F), bf16),
                pltpu.VMEM((D // W, T, W), bf16),
                pltpu.VMEM((D // W, T // 2, W), bf16),
                pltpu.VMEM((R, F), jnp.float32),
                pltpu.VMEM((R, F), jnp.float32),
                pltpu.VMEM((1, R), jnp.float32),
                pltpu.SemaphoreType.DMA((4,)),
                pltpu.SemaphoreType.DMA((n_tp,)),
                pltpu.SemaphoreType.DMA((n_tp,)),
                pltpu.SemaphoreType.DMA((2, S)),
                pltpu.SemaphoreType.DMA((2, S)),
                pltpu.SemaphoreType.DMA((D // W,)),
                pltpu.SemaphoreType.DMA((D // W,)),
                pltpu.SemaphoreType.DMA((D // W,)),
                pltpu.SemaphoreType.DMA((n_tp // 2 + 1, Dk // W, 2)),
            ],
            compiler_params=pltpu.CompilerParams(
                collective_id=0, has_side_effects=True, vmem_limit_bytes=44 * 2**20
            ),
        )(tokens, norm_gain[None, :], up_master, down_master)
        return pl.pallas_call(
            finish_kernel,
            out_shape=(
                jax.ShapeDtypeStruct((D, F), bf16),
                jax.ShapeDtypeStruct((F, D), bf16),
                jax.ShapeDtypeStruct((T, Dk), bf16),
            ),
            in_specs=[vmem_spec] * 3,
            out_specs=(any_spec,) * 3,
            scratch_shapes=[pltpu.VMEM((T, Dk), bf16), pltpu.SemaphoreType.DMA((3,))],
            compiler_params=pltpu.CompilerParams(vmem_limit_bytes=8 * 2**20),
        )(up_v, dn_v, recv)

    in_specs = (P("fs", "tp"), P("fs"), P("fs", "tp"), P("fs", "tp"))
    out_specs = (P(None, "tp"), P("tp", None), P("fs", "tp"))
    return jax.shard_map(on_device, mesh=mesh, in_specs=in_specs, out_specs=out_specs, check_vma=False)
```
